32 devices in a mesh: grp: 2 (over y), fs: 4 (over z), tp: 4 (over x, core).
Axes of the slice: x: 2, y: 2, z: 4, core: 2. Of those that a mesh axis runs over, the one named last changes fastest.
Arguments:
- tokens: bfloat16 [1792, 2048], P(('grp', 'fs'), 'tp'), parts along dimension 0, may hold values from -6 to 6
- route_ids: int32 [1792, 2], P(('grp', 'fs')), parts along dimension 0, may hold values from 0 to 3, all different within a row; in each aligned block of 224 rows (0 to 223, 224 to 447, ...) at most 168 rows name the same one
- route_weights: float32 [1792, 2], P(('grp', 'fs')), parts along dimension 0, may hold values from 0.25 to 1
- norm_gain: float32 [2048], P('fs'), may hold values from 0.1 to 1.9
- gate_master: float32 [4, 2048, 512], P(None, 'fs', 'tp'), may hold values from -0.125 to 0.125
- up_master: float32 [4, 2048, 512], P(None, 'fs', 'tp'), may hold values from -0.125 to 0.125
- down_master: float32 [4, 2048, 512], P(None, 'fs', 'tp'), may hold values from -0.25 to 0.25
Outputs:
- gate_serve: bfloat16 [8, 2048, 512], P(('grp', 'fs'), None, 'tp'), parts along dimension 0
- up_serve: bfloat16 [8, 2048, 512], P(('grp', 'fs'), None, 'tp'), parts along dimension 0
- down_serve: bfloat16 [8, 2048, 512], P(('grp', 'fs'), None, 'tp'), parts along dimension 0
- moe_output: bfloat16 [1792, 2048], P(('grp', 'fs'), 'tp'), parts along dimension 0
The draws below stay inside these ranges and needn't reach their ends.
There are 2 independent parts, one for each index of `grp`. The reference program is written for one: setup_inputs(seed, part) draws one part's arguments, and reference() takes and returns one part's arrays. A program takes and returns all parts, laid end to end along the dimension named above; an argument that names none is the same for every part. Nothing has to cross between parts.
Inputs may be any that keep to these rules, and one draw needn't show every extreme that they name: `route_ids`: the 2 experts of a row differ; within the rows of one index of fs (aligned blocks of 224 rows) no expert is named more than 168 times.
All inputs are finite; a program needn't handle non-finite values.
Results may differ from the reference program's by a relative error of at most 0.012.
Values may be sent and summed in bfloat16 or wider, within the bound.
A program may use at most 64 MiB of HBM per device.

```python
import math
import jax
import jax.numpy as jnp
import numpy as np
from jax import lax

D = 2048
F = 512
TOP = 2
TOK_DEV = 224
EXPERTS = 4
TOKENS = 896
CAP = 168
N_FS = 4
N_TP = 4


def block_levels(stream_key, extent, split, smallest, top_value):
    def one(dim, shards_of):
        steps = jax.random.uniform(jax.random.fold_in(jax.random.fold_in(stream_key, 6), dim), (shards_of,), jnp.float32, smallest / len(split), top_value / len(split))
        return jnp.repeat(jnp.exp(steps), extent[dim] // shards_of).reshape((-1,) + (1,) * (len(extent) - dim - 1))

    level = one(*split[0])
    for cut in split[1:]:
        level = level * one(*cut)
    return level


def deal_out(stream_key, own, number, rows, number_of, top, bound, lean):
    ranking = jax.random.permutation(stream_key, number_of)
    crowded, ordinary = portions_of(number_of, rows * top, bound, lean, True), portions_of(number_of, rows * top, bound, lean, False)
    places = jnp.arange(number_of)

    def named(sizes, turn):
        used = int((sizes > 0).sum())
        fixed = max(1, used // 4)
        passed = fixed + (places - fixed + turn * (used - fixed)) % max(1, number_of - fixed)
        return jnp.zeros((number_of,), jnp.int32).at[ranking[jnp.where(places < fixed, places, passed)]].set(jnp.asarray(sizes, jnp.int32))

    sizes = jnp.where(number % 4 == 0, named(crowded, number // 4), named(ordinary, number - number // 4 - 1))
    mixed = jax.random.permutation(jax.random.fold_in(own, 3), number_of)
    donor, taker = mixed[0:number_of // 2 * 2:2], mixed[1:number_of // 2 * 2:2]
    margin = jnp.minimum(sizes[donor] - 1, bound - sizes[taker]) // 2
    margin = jnp.where((donor == ranking[0]) | (taker == ranking[0]) | (sizes[taker] == 0), 0, jnp.maximum(margin, 0))
    passed = jax.random.randint(jax.random.fold_in(own, 4), (number_of // 2,), 0, 1 << 20) % (margin + 1)
    sizes = sizes.at[donor].add(-passed).at[taker].add(passed)
    members = jnp.searchsorted(jnp.cumsum(sizes), jnp.arange(rows * top), side="right").astype(jnp.int32)
    listing = members.reshape(top, rows).T
    listing = listing[jax.random.permutation(jax.random.fold_in(own, 1), rows)]
    turn = jax.random.randint(jax.random.fold_in(own, 2), (rows, 1), 0, top)
    return jnp.take_along_axis(listing, (jnp.arange(top)[None, :] + turn) % top, axis=1)


def portions_of(number_of, total, limit, slope, full):
    loads = [(1 << 20) // math.isqrt(rank ** slope) + 1 for rank in range(1, number_of + 1)]
    largest = limit if full else min(limit, max(-(-total // number_of), total * loads[0] // sum(loads)))
    least = 1 if total - largest >= number_of - 1 else 0
    counts, spare = [largest] + [least] * (number_of - 1), total - largest - least * (number_of - 1)
    while spare > 0:
        candidates = [i for i in range(1, number_of) if counts[i] < largest] or [i for i in range(1, number_of) if counts[i] < limit]
        mass, budget = sum([loads[i] for i in candidates]), spare
        for i in candidates:
            more = min(limit - counts[i], max(1, budget * loads[i] // mass), spare)
            counts[i] = counts[i] + more
            spare = spare - more
    return np.array(counts)


def centred(rng, shape, deviation, limit, cuts=(), kind=jnp.bfloat16):
    values = deviation * jax.random.normal(rng, shape, jnp.float32)
    if cuts:
        values = values * block_levels(rng, shape, cuts, -0.22, 0.18)
    return jnp.clip(values, -limit, limit).astype(kind)


def setup_inputs(seed: int = 0, part: int = 0) -> dict:
    key_list = jax.random.split(jax.random.key(seed), 8)
    part_splits = jax.random.split(jax.random.fold_in(key_list[7], part), 8)
    tokens = centred(part_splits[0], (TOKENS, D), 1.0, 6.0, ((0, 4), (1, 4)))
    route_ids_keys = jax.random.split(jax.random.fold_in(part_splits[1], 1), TOKENS // TOK_DEV)
    route_ids_turns = jax.random.permutation(jax.random.fold_in(part_splits[1], 3), TOKENS // TOK_DEV)
    route_ids = jax.vmap(lambda own, number: deal_out(jax.random.fold_in(part_splits[1], 2), own, number, TOK_DEV, EXPERTS, TOP, CAP, 1))(route_ids_keys, route_ids_turns).reshape((TOKENS, TOP))
    route_weights = jnp.clip(0.25 + 0.75 * jax.random.uniform(part_splits[2], (TOKENS, TOP), jnp.float32) ** block_levels(part_splits[2], (TOKENS, TOP), ((0, 4),), -0.2, 0.2), 0.25, 1.0)
    norm_gain = jnp.clip(1.0 + 0.18 * jax.random.normal(key_list[3], (D,), jnp.float32), 0.1, 1.9)
    gate_master = centred(key_list[4], (EXPERTS, D, F), D ** -0.5, 0.125, ((1, 4), (2, 4)), jnp.float32)
    up_master = centred(key_list[5], (EXPERTS, D, F), D ** -0.5, 0.125, ((1, 4), (2, 4)), jnp.float32)
    down_master = centred(key_list[6], (EXPERTS, D, F), F ** -0.5, 0.25, ((1, 4), (2, 4)), jnp.float32)
    return {"tokens": tokens, "route_ids": route_ids, "route_weights": route_weights, "norm_gain": norm_gain, "gate_master": gate_master, "up_master": up_master, "down_master": down_master}


norm_epsilon = 1e-06

def slot_numbers(route_ids, experts, capacity):
    flat_ids = route_ids.reshape(-1)
    onehot = (flat_ids[:, None] == jnp.arange(experts, dtype=jnp.int32)[None, :]).astype(jnp.int32)
    before = jnp.cumsum(onehot, axis=0) - onehot
    position = lax.optimization_barrier(jnp.sum(before * onehot, axis=1))
    return (flat_ids * capacity + position).astype(jnp.int32).reshape(route_ids.shape)

def reference(tokens, route_ids, route_weights, norm_gain, gate_master, up_master, down_master):
    row_gain = norm_gain[None, :, None]
    gate_serve = (gate_master * row_gain).astype(jnp.bfloat16)
    up_serve = (up_master * row_gain).astype(jnp.bfloat16)
    down_serve = down_master.astype(jnp.bfloat16)
    values = tokens.astype(jnp.float32)
    normed = (values * lax.rsqrt(lax.optimization_barrier(jnp.mean(values * values, axis=1, keepdims=True)) + norm_epsilon)).astype(jnp.bfloat16)
    blocks = normed.reshape(N_FS, TOK_DEV, D)
    expert_ids = route_ids.reshape(N_FS, TOK_DEV, TOP).astype(jnp.int32)
    slot_ids = jax.vmap(lambda ids: slot_numbers(ids, EXPERTS, CAP))(expert_ids)
    block_index = jnp.broadcast_to(jnp.arange(N_FS, dtype=jnp.int32)[:, None, None], slot_ids.shape)
    token_rows = jnp.broadcast_to(blocks[:, :, None, :], (N_FS, TOK_DEV, TOP, D))
    buffer = jnp.zeros((N_FS, EXPERTS * CAP, D), jnp.bfloat16).at[block_index, slot_ids].set(token_rows)
    by_expert = jnp.moveaxis(buffer.reshape(N_FS, EXPERTS, CAP, D), 1, 0)

    def expert_out(inputs):
        rows, gate_w, up_w, down_w = inputs
        flat_rows = rows.reshape(N_FS * CAP, D)
        gate_sum = jnp.dot(flat_rows, gate_w, preferred_element_type=jnp.float32)
        up_sum = jnp.dot(flat_rows, up_w, preferred_element_type=jnp.float32)
        hidden = (jax.nn.silu(gate_sum) * up_sum).astype(jnp.bfloat16)
        parts_hidden = hidden.astype(jnp.float32).reshape(N_FS * CAP, N_TP, F // N_TP)
        parts_down = down_w.astype(jnp.float32).reshape(D, N_TP, F // N_TP)
        partial_value = jnp.einsum('rpf,dpf->prd', parts_hidden, parts_down)
        rounded = lax.optimization_barrier(partial_value.astype(jnp.bfloat16)).astype(jnp.float32)
        return lax.optimization_barrier(jnp.sum(rounded, axis=0)).astype(jnp.bfloat16).reshape(N_FS, CAP, D)
    outputs = lax.map(expert_out, (by_expert, gate_serve, up_serve, down_serve))
    position = slot_ids - expert_ids * CAP
    picked = outputs[expert_ids, block_index, position]
    weights = route_weights.reshape(N_FS, TOK_DEV, TOP)[..., None]
    combined = lax.optimization_barrier(jnp.sum(weights * picked.astype(jnp.float32), axis=2))
    return (gate_serve, up_serve, down_serve, combined.reshape(TOKENS, D).astype(jnp.bfloat16))
```

```python
import jax
import jax.numpy as jnp
from jax import lax
from jax.experimental import pallas as pl
from jax.experimental.pallas import tpu as pltpu
from jax.sharding import PartitionSpec as P

norm_epsilon = 1e-06


def slot_numbers(route_ids, experts, capacity):
    flat_ids = route_ids.reshape(-1)
    onehot = (flat_ids[:, None] == jnp.arange(experts, dtype=jnp.int32)[None, :]).astype(jnp.int32)
    before = jnp.cumsum(onehot, axis=0) - onehot
    position = jnp.sum(before * onehot, axis=1)
    return (flat_ids * capacity + position).reshape(route_ids.shape)


def local(tokens, route_ids, route_weights, norm_gain, gate_master, up_master, down_master):
    experts = gate_master.shape[0]
    shards = lax.axis_size("fs")
    columns = lax.axis_size("tp")
    per_device = experts // shards
    tok_rows = route_ids.shape[0]
    top_count = route_ids.shape[1]
    local_width = tokens.shape[1]
    model_width = local_width * columns
    capacity = max(2, 3 * tok_rows * top_count // (2 * experts))
    row_gain = norm_gain[None, :, None]
    gate_half = (gate_master * row_gain).astype(jnp.bfloat16)
    up_half = (up_master * row_gain).astype(jnp.bfloat16)
    down_half = down_master.astype(jnp.bfloat16)
    gate_serve, up_serve, down_serve = (
        lax.all_to_all(gate_half, "fs", split_axis=0, concat_axis=1, tiled=True),
        lax.all_to_all(up_half, "fs", split_axis=0, concat_axis=1, tiled=True),
        lax.all_to_all(down_half, "fs", split_axis=0, concat_axis=1, tiled=True),
    )
    slot_ids = slot_numbers(route_ids, experts, capacity)
    slot_range = jnp.arange(experts * capacity, dtype=jnp.int32)
    selects = [
        (slot_ids[:, rank_slot, None] == slot_range[None, :]).astype(jnp.bfloat16)
        for rank_slot in range(top_count)
    ]
    placing = selects[0]
    for extra in selects[1:]:
        placing = placing + extra
    local_values = tokens.astype(jnp.float32)
    squares = lax.psum(jnp.sum(local_values * local_values, axis=1), "tp")
    inverse = lax.rsqrt(squares / model_width + norm_epsilon)[:, None]
    normed = (local_values * inverse).astype(jnp.bfloat16)
    buffer = jnp.einsum("ts,td->sd", placing, normed, preferred_element_type=jnp.float32).astype(
        jnp.bfloat16
    )
    arrived = lax.all_to_all(
        buffer.reshape(shards, per_device * capacity, local_width),
        "fs",
        split_axis=0,
        concat_axis=0,
        tiled=True,
    )
    arrived = arrived.reshape(shards, per_device, capacity, local_width)
    partial_value = lax.all_gather(arrived, "tp", axis=3, tiled=True)
    gate_sum = jnp.einsum(
        "sxcd,xdf->xscf", partial_value, gate_serve, preferred_element_type=jnp.float32
    )
    up_sum = jnp.einsum(
        "sxcd,xdf->xscf", partial_value, up_serve, preferred_element_type=jnp.float32
    )
    hidden = (jax.nn.silu(gate_sum) * up_sum).astype(jnp.bfloat16)
    products = jnp.einsum("xdf,xscf->dsxc", down_serve, hidden, preferred_element_type=jnp.float32)
    summed = lax.psum_scatter(
        products.reshape(local_width * lax.axis_size("tp"), shards * per_device * capacity).astype(
            jnp.bfloat16
        ),
        "tp",
        scatter_dimension=0,
        tiled=True,
    )
    returned = lax.all_to_all(
        summed.reshape(local_width, shards, per_device * capacity),
        "fs",
        split_axis=1,
        concat_axis=1,
        tiled=True,
    )
    returned = returned.reshape(local_width, experts * capacity)
    combined = jnp.zeros((tok_rows, local_width), jnp.float32)
    for rank_slot in range(top_count):
        picked = jnp.einsum(
            "ts,ds->td", selects[rank_slot], returned, preferred_element_type=jnp.float32
        )
        combined = combined + route_weights[:, rank_slot : rank_slot + 1] * picked
    return (gate_serve, up_serve, down_serve, combined.astype(jnp.bfloat16))


MESH = pl.DeviceIdType.MESH
bf16, f32, i32 = jnp.bfloat16, jnp.float32, jnp.int32
GU_CUT, DN_CUT = 2, 4


def remote(src, dst, send, recv, to):
    return pltpu.make_async_remote_copy(
        src_ref=src, dst_ref=dst, send_sem=send, recv_sem=recv, device_id=to, device_id_type=MESH
    )


def kernel(
    tokens, ids_h, weights_h, gain_h, gm, um, dm,
    wgu, wd, moe,
    xt, ids, weights, gain, gcol, mv, sgu, sd, acc, inv, scale, wrow, wsend, hid,
    ss, sr, xs, xr, keep, zs, zr,
    in_sem, ld_sem, c_send, c_recv, w_send, w_recv, p_sib, p_x, p_recv,
    gu_send, gu_recv, guy_send, guy_recv, dn_send, dn_recv, dny_send, dny_recv,
    s_send, s_recv, x_send, x_recv, z_send, z_recv,
):
    g, f, t = lax.axis_index("grp"), lax.axis_index("fs"), lax.axis_index("tp")
    H, Fl = mv.shape[2:]
    Dl = 2 * H
    T, Dq = tokens.shape
    NT = xt.shape[0]
    D = NT * Dq
    Rg, Rd = H // GU_CUT, H // DN_CUT
    units = Dl // Fl
    per_half = units // 2
    pair, me = f // 2, lax.rem(f, 2)
    chip, core = t // 2, lax.rem(t, 2)
    mate = f + 1 - 2 * me
    twin = f + 2 - 4 * pair
    mate_twin = mate + 2 - 4 * pair
    far_a, far_b = 2 - pair, 3 - 3 * pair
    sib, over = {"tp": t + 1 - 2 * core}, {"tp": t + 2 - 4 * chip}
    peer, to_mate = {"grp": 1 - g}, {"fs": mate}
    mine_rows, mate_rows = (pl.ds(pl.multiple_of(i * T, T), T) for i in (me, 1 - me))
    inner = (f + 1) // 2 % 2 == 1
    home = chip == pair

    def cut(s, half, p, n):
        return pl.ds(pl.multiple_of(s * Dl + half * H + p * n, n), n)

    def both(s):
        return pl.ds(pl.multiple_of(s * Dl, Dl), Dl)

    small = [
        pltpu.make_async_copy(gain_h, gain, in_sem.at[0]),
        pltpu.make_async_copy(tokens, xt.at[t, mine_rows, :], in_sem.at[1]),
        pltpu.make_async_copy(ids_h, ids, in_sem.at[2]),
        pltpu.make_async_copy(weights_h, weights, in_sem.at[3]),
    ]
    small[0].start()
    small[1].start()
    picks = [
        (1 - me, g), (1 - me + 2, g), (me, g), (me + 2, g), (me, 1 - g), (me + 2, 1 - g),
    ]
    loads = {}
    for k, m in [(k, m) for k in (0, 2, 1, 3) for m in (0, 1)] + [
        (k, 2) for k in (0, 1, 2, 3)
    ] + [(k, m) for k in (4, 5) for m in (0, 1, 2)]:
        e, half = picks[k]
        loads[k, m] = pltpu.make_async_copy(
            (gm, um, dm)[m].at[e, pl.ds(pl.multiple_of(half * H, H), H), :],
            mv.at[m, k], ld_sem.at[m, k],
        )
        loads[k, m].start()
    small[2].start()
    small[3].start()

    barrier = pltpu.get_barrier_semaphore()
    friends = [to_mate, {"fs": twin}, {"fs": mate_twin}, peer, sib, over]
    for who in friends:
        pl.semaphore_signal(barrier, inc=1, device_id=who, device_id_type=MESH)

    small[0].wait()
    gcol[...] = jnp.transpose(jnp.broadcast_to(gain[...], (Fl, Dl)))
    mine_half = pl.ds(pl.multiple_of(g * H, H), H)
    other_half = pl.ds(pl.multiple_of((1 - g) * H, H), H)
    small[1].wait()
    pl.semaphore_wait(barrier, len(friends))

    def tok(q, rows):
        return xt.at[q, rows, :]

    token_hop = remote(tok(t, mine_rows), tok(t, mine_rows), c_send, c_recv, to_mate)
    token_hop.start()

    def spread(rows, i):
        block = tok(t, rows)
        remote(block, block, p_x.at[i], p_recv.at[t, i], over).start()
        remote(block, block, p_sib.at[t, i], p_recv.at[t, i], sib).start()

    def pass_on(rows, i):
        q = t + 2 - 4 * chip
        block = tok(q, rows)
        remote(block, block, p_recv.at[q, i], p_recv.at[q, i], sib).wait_recv()
        remote(block, block, p_sib.at[q, i], p_recv.at[q, i], sib).start()

    def sib_arrived(rows, i):
        for c in range(2):
            q = 2 * c + 1 - core
            block = tok(q, rows)
            remote(block, block, p_recv.at[q, i], p_recv.at[q, i], sib).wait_recv()

    spread(mine_rows, me)

    def gu_copy(kind, slot, p):
        src = (
            wgu.at[slot, cut(f, g, p, Rg), :] if kind == 0 else sgu.at[slot, p * Rg : (p + 1) * Rg, :]
        )
        return remote(
            src, wgu.at[slot, cut(f, g, p, Rg), :], gu_send.at[kind, slot, p],
            gu_recv.at[f, slot, p], {"fs": (twin, mate_twin, mate)[kind]},
        )

    def dn_copy(kind, p):
        src = wd.at[cut(f, g, p, Rd), :] if kind == 0 else sd.at[p * Rd : (p + 1) * Rd, :]
        return remote(
            src, wd.at[cut(f, g, p, Rd), :], dn_send.at[kind, p], dn_recv.at[f, p],
            {"fs": (twin, mate_twin, mate)[kind]},
        )

    def send_gu(slot, kinds):
        for p in range(GU_CUT):
            for kind in kinds:
                gu_copy(kind, slot, p).start()

    def send_dn(kinds):
        for p in range(DN_CUT):
            for kind in kinds:
                dn_copy(kind, p).start()

    def gu_ready(slot, k, dst, part):
        loads[k, 0].wait()
        loads[k, 1].wait()
        dst[:, :Fl] = (mv[0, k] * gcol[part, :]).astype(bf16)
        dst[:, Fl:] = (mv[1, k] * gcol[part, :]).astype(bf16)

    own_gu = [wgu.at[slot, cut(f, g, 0, H), :] for slot in range(2)]
    gu_ready(0, 0, sgu.at[0], mine_half)

    @pl.when(inner)
    def _():
        send_gu(0, (1, 2))

    @pl.when(jnp.logical_not(inner))
    def _():
        send_gu(0, (2,))

    gu_ready(0, 2, own_gu[0], mine_half)

    @pl.when(inner)
    def _():
        send_gu(0, (0,))

    gu_ready(1, 1, sgu.at[1], mine_half)

    @pl.when(inner)
    def _():
        send_gu(1, (1, 2))

    @pl.when(jnp.logical_not(inner))
    def _():
        send_gu(1, (2,))

    gu_ready(1, 3, own_gu[1], mine_half)

    @pl.when(inner)
    def _():
        send_gu(1, (0,))

    @pl.when(jnp.logical_not(inner))
    def _():
        send_gu(0, (0, 1))
        send_gu(1, (0, 1))

    for k in range(4):
        loads[k, 2].wait()
    for slot in range(2):
        lanes = slice(slot * Fl, (slot + 1) * Fl)
        sd[:, lanes] = mv[2, slot].astype(bf16)
        wd[cut(f, g, 0, H), lanes] = mv[2, 2 + slot].astype(bf16)
    send_dn((2,))

    @pl.when(jnp.logical_not(inner))
    def _():
        send_dn((0, 1))

    for slot in range(2):
        lanes = slice(slot * Fl, (slot + 1) * Fl)
        gu_ready(slot, 4 + slot, wgu.at[slot, cut(f, 1 - g, 0, H), :], other_half)
        loads[4 + slot, 2].wait()
        wd[cut(f, 1 - g, 0, H), lanes] = mv[2, 4 + slot].astype(bf16)

    small[2].wait()
    small[3].wait()
    wrow[me] = jnp.zeros(wsend.shape, f32)
    wsend[...] = jnp.zeros(wsend.shape, f32)
    for slot in range(2):
        for ref, parity in ((wrow.at[me], me), (wsend, 1 - me)):
            row = jnp.where(ids[...] == parity + 2 * slot, weights[...], 0.0)
            ref[slot : slot + 1, :T] = jnp.sum(row, axis=0, keepdims=True)
    w_hop = remote(wsend, wrow.at[me], w_send, w_recv, to_mate)
    w_hop.start()

    remote(tok(t, mate_rows), tok(t, mate_rows), c_send, c_recv, to_mate).wait_recv()
    spread(mate_rows, 1 - me)

    def gu_forward(s, slot, p):
        here = wgu.at[slot, cut(s, g, p, Rg), :]
        remote(here, here, gu_recv.at[s, slot, p], gu_recv.at[s, slot, p], peer).wait_recv()
        remote(here, here, guy_send.at[s, slot, p], guy_recv.at[s, slot, p], peer).start()

    def gu_peer(s, slot):
        for p in range(GU_CUT):
            there = wgu.at[slot, cut(s, 1 - g, p, Rg), :]
            remote(there, there, guy_recv.at[s, slot, p], guy_recv.at[s, slot, p], peer).wait_recv()

    def dn_forward(s, p):
        here = wd.at[cut(s, g, p, Rd), :]
        remote(here, here, dn_recv.at[s, p], dn_recv.at[s, p], peer).wait_recv()
        remote(here, here, dny_send.at[s, p], dny_recv.at[s, p], peer).start()

    def dn_peer(s, p):
        there = wd.at[cut(s, 1 - g, p, Rd), :]
        remote(there, there, dny_recv.at[s, p], dny_recv.at[s, p], peer).wait_recv()

    def gu_all(s, slot):
        for p in range(GU_CUT):
            gu_forward(s, slot, p)

    def partial_sums(s, slot):
        return jnp.dot(xt[s], wgu[slot, both(s), :], preferred_element_type=f32)

    gu_all(mate, 0)
    gu_all(far_a, 0)
    pass_on(mine_rows, me)
    gu_all(mate, 1)
    gu_all(far_a, 1)
    pass_on(mate_rows, 1 - me)

    remote(wsend, wrow.at[1 - me], w_recv, w_recv, to_mate).wait_recv()
    sib_arrived(mine_rows, me)
    sib_arrived(mate_rows, 1 - me)
    for i in range(2):
        rows = slice(i * T, (i + 1) * T)
        sq = jnp.zeros((T, Fl), f32)
        for q in range(NT):
            for c in range(Dq // Fl):
                part = xt[q, rows, c * Fl : (c + 1) * Fl].astype(f32)
                sq = sq + part * part
        root = lax.rsqrt(jnp.sum(sq, axis=1, keepdims=True) / D + norm_epsilon)
        inv[rows, :] = jnp.broadcast_to(root, (T, Fl))
        for slot in range(2):
            wide = jnp.transpose(
                jnp.broadcast_to(wrow[i, slot : slot + 1, :], (Fl, wrow.shape[2]))
            )
            scale[slot, rows, :] = wide[:T] * root

    for slot in range(2):
        acc[slot] = partial_sums(f, slot)
    for slot in range(2):
        for s in (mate, far_a):
            gu_peer(s, slot)
            acc[slot] += partial_sums(s, slot)

    gu_all(far_b, 0)
    gu_forward(far_b, 1, 0)

    @pl.when(inner)
    def _():
        send_dn((0, 1))

    for p in range(1, GU_CUT):
        gu_forward(far_b, 1, p)
    for p in range(DN_CUT):
        dn_forward(mate, p)

    for slot in range(2):
        gu_peer(far_b, slot)
        sums = acc[slot] + partial_sums(far_b, slot)
        gate, up = sums[:, :Fl] * inv[...], sums[:, Fl:] * scale[slot]
        hid[:, slot * Fl : (slot + 1) * Fl] = (gate / (1.0 + jnp.exp(-gate)) * up).astype(bf16)

    near_mine, near_theirs = 2 * pair + core, 2 * pair + 1 - core
    far_mine, far_theirs = 2 - 2 * pair + core, 2 - 2 * pair + 1 - core

    def out_part(s, u, n):
        rows = pl.ds(pl.multiple_of(s * Dl + u * Fl, Fl), n * Fl)
        return lax.dot_general(
            hid[...], wd[rows, :], (((1,), (1,)), ((), ())), preferred_element_type=f32
        )

    def swap(n, u, count):
        at = pl.ds(u, count)
        return remote(ss.at[n, at], sr.at[n, at], s_send.at[n, u], s_recv.at[n, u], sib)

    def cross(u, count):
        at = pl.ds(u, count)
        return remote(xs.at[at], xr.at[at], x_send.at[u], x_recv.at[u], over)

    def back(u, count):
        at = pl.ds(u, count)
        return remote(zs.at[at], zr.at[at], z_send.at[u], z_recv.at[u], to_mate)

    def theirs(n, s, u, count):
        y = out_part(s, u, count)
        for j in range(count):
            ss[n, u + j] = y[:, j * Fl : (j + 1) * Fl].astype(bf16)
        swap(n, u, count).start()

    def mine(n, s, u, count):
        y = out_part(s, u, count)
        swap(n, u, count).wait_recv()
        kept = home if n == 0 else jnp.logical_not(home)
        parts = [y[:, j * Fl : (j + 1) * Fl] + sr[n, u + j].astype(f32) for j in range(count)]

        @pl.when(kept)
        def _():
            for j in range(count):
                keep[u + j] = parts[j]

        @pl.when(jnp.logical_not(kept))
        def _():
            for j in range(count):
                xs[u + j] = parts[j].astype(bf16)
            cross(u, count).start()

    def give_back(u, count):
        cross(u, count).wait_recv()
        for j in range(count):
            zs[u + j] = (keep[u + j, mate_rows, :] + xr[u + j, mate_rows, :].astype(f32)).astype(bf16)
        back(u, count).start()

    def finish(u, count):
        back(u, count).wait_recv()
        for j in range(count):
            lane = (u + j) * Fl
            lanes = pl.ds(lane if isinstance(lane, int) else pl.multiple_of(lane, Fl), Fl)
            moe[:, lanes] = (
                keep[u + j, mine_rows, :] + xr[u + j, mine_rows, :].astype(f32) + zr[u + j].astype(f32)
            ).astype(bf16)

    ratio = DN_CUT // per_half

    def far_forward(j):
        for p in range(j * ratio, (j + 1) * ratio):
            dn_forward(far_a, p)
            dn_forward(far_b, p)

    def far_peer(j):
        for p in range(j * ratio, (j + 1) * ratio):
            dn_peer(far_a, p)
            dn_peer(far_b, p)

    for p in range(DN_CUT):
        dn_peer(mate, p)
    for h in range(2):
        theirs(0, near_theirs, h * per_half, per_half)
    for h in range(2):
        mine(0, near_mine, h * per_half, per_half)

    for j in range(per_half):
        far_forward(j)
        for half in (g, 1 - g):
            u = half * per_half + j
            if half is not g:
                far_peer(j)
            theirs(1, far_theirs, u, 1)
            mine(1, far_mine, u, 1)
        if j == 0:
            @pl.when(home)
            def _():
                for h in range(2):
                    give_back(h * per_half, per_half)

    @pl.when(home)
    def _():
        for h in range(2):
            finish(h * per_half, per_half)

    @pl.when(jnp.logical_not(home))
    def _():
        order = [half * per_half + j for j in range(per_half) for half in (g, 1 - g)]
        for u in order:
            give_back(u, 1)
        for u in order:
            finish(u, 1)

    token_hop.wait_send()
    w_hop.wait_send()
    for i, rows in ((me, mine_rows), (1 - me, mate_rows)):
        block = tok(t, rows)
        remote(block, block, p_x.at[i], p_x.at[i], over).wait_send()
        for q in (t, t + 2 - 4 * chip):
            remote(block, block, p_sib.at[q, i], p_sib.at[q, i], sib).wait_send()
    for kind in range(3):
        for slot in range(2):
            for p in range(GU_CUT):
                gu_copy(kind, slot, p).wait_send()
        for p in range(DN_CUT):
            dn_copy(kind, p).wait_send()
    for s in (mate, far_a, far_b):
        for slot in range(2):
            for p in range(GU_CUT):
                here = wgu.at[slot, cut(s, g, p, Rg), :]
                remote(here, here, guy_send.at[s, slot, p], guy_send.at[s, slot, p], peer).wait_send()
        for p in range(DN_CUT):
            here = wd.at[cut(s, g, p, Rd), :]
            remote(here, here, dny_send.at[s, p], dny_send.at[s, p], peer).wait_send()
    for h in range(2):
        swap(0, h * per_half, per_half).wait_send()
    for u in range(units):
        swap(1, u, 1).wait_send()

    @pl.when(home)
    def _():
        for u in range(units):
            cross(u, 1).wait_send()
        for h in range(2):
            back(h * per_half, per_half).wait_send()

    @pl.when(jnp.logical_not(home))
    def _():
        for h in range(2):
            cross(h * per_half, per_half).wait_send()
        for u in range(units):
            back(u, 1).wait_send()


def finish_kernel(wgu, wd, moe, gate_o, up_o, down_o, moe_o, sems):
    Fl = gate_o.shape[2]
    slot = lax.axis_index("fs") // 2
    lanes = pl.ds(pl.multiple_of(slot * Fl, Fl), Fl)
    copies = [
        pltpu.make_async_copy(wgu.at[slot, :, :Fl], gate_o.at[0], sems.at[0]),
        pltpu.make_async_copy(wgu.at[slot, :, Fl:], up_o.at[0], sems.at[1]),
        pltpu.make_async_copy(wd.at[:, lanes], down_o.at[0], sems.at[2]),
        pltpu.make_async_copy(moe, moe_o, sems.at[3]),
    ]
    for cp in copies:
        cp.start()
    for cp in copies:
        cp.wait()


def fused(tokens, route_ids, route_weights, norm_gain, gate_master, up_master, down_master):
    NF, NT = lax.axis_size("fs"), lax.axis_size("tp")
    E, Dl, Fl = gate_master.shape
    T, Dq = tokens.shape
    K = route_ids.shape[1]
    H = Dl // 2
    D = Dl * NF
    Tw = -(-T // 128) * 128
    units = Dl // Fl
    dma = pltpu.SemaphoreType.DMA
    vmem, hbm = pl.BlockSpec(memory_space=pltpu.VMEM), pl.BlockSpec(memory_space=pl.ANY)
    gu, dn = (NF, 2, GU_CUT), (NF, DN_CUT)
    ins = (
        tokens, route_ids.T, route_weights.T, norm_gain[None, :],
        gate_master, up_master, down_master,
    )
    done = pl.pallas_call(
        kernel,
        out_shape=(
            pltpu.VMEM((2, D, 2 * Fl), bf16), pltpu.VMEM((D, 2 * Fl), bf16), pltpu.VMEM((T, Dq), bf16),
        ),
        in_specs=[hbm] * 7,
        out_specs=(vmem,) * 3,
        scratch_shapes=[
            pltpu.VMEM((NT, 2 * T, Dq), bf16),
            pltpu.VMEM((K, T), i32),
            pltpu.VMEM((K, T), f32),
            pltpu.VMEM((1, Dl), f32),
            pltpu.VMEM((Dl, Fl), f32),
            pltpu.VMEM((3, 6, H, Fl), f32),
            pltpu.VMEM((2, H, 2 * Fl), bf16),
            pltpu.VMEM((H, 2 * Fl), bf16),
            pltpu.VMEM((2, 2 * T, 2 * Fl), f32),
            pltpu.VMEM((2 * T, Fl), f32),
            pltpu.VMEM((2, 2 * T, Fl), f32),
            pltpu.VMEM((2, 8, Tw), f32),
            pltpu.VMEM((8, Tw), f32),
            pltpu.VMEM((2 * T, 2 * Fl), bf16),
            pltpu.VMEM((2, units, 2 * T, Fl), bf16),
            pltpu.VMEM((2, units, 2 * T, Fl), bf16),
            pltpu.VMEM((units, 2 * T, Fl), bf16),
            pltpu.VMEM((units, 2 * T, Fl), bf16),
            pltpu.VMEM((units, 2 * T, Fl), f32),
            pltpu.VMEM((units, T, Fl), bf16),
            pltpu.VMEM((units, T, Fl), bf16),
            dma((4,)), dma((3, 6)),
            dma(()), dma(()), dma(()), dma(()),
            dma((NT, 2)), dma((2,)), dma((NT, 2)),
            dma((3, 2, GU_CUT)), dma(gu), dma(gu), dma(gu),
            dma((3, DN_CUT)), dma(dn), dma(dn), dma(dn),
            dma((2, units)), dma((2, units)),
            dma((units,)), dma((units,)),
            dma((units,)), dma((units,)),
        ],
        compiler_params=pltpu.CompilerParams(
            collective_id=0, has_side_effects=True, vmem_limit_bytes=48 * 1024 * 1024
        ),
    )(*[pltpu.with_memory_space_constraint(a, pltpu.HBM) for a in ins])
    serve = jax.ShapeDtypeStruct((1, D, Fl), bf16)
    return pl.pallas_call(
        finish_kernel,
        out_shape=(serve, serve, serve, jax.ShapeDtypeStruct((T, Dq), bf16)),
        in_specs=[vmem] * 3,
        out_specs=(hbm,) * 4,
        scratch_shapes=[dma((4,))],
    )(*[pltpu.with_memory_space_constraint(a, pltpu.VMEM) for a in done])


def solution(mesh):
    shape = mesh.shape
    fits = shape['grp'] == 2 and shape['tp'] == shape['fs'] == 4
    body = fused if fits else local
    placed = (
        P(("grp", "fs"), "tp"),
        P(("grp", "fs"), None),
        P(("grp", "fs"), None),
        P("fs"),
        P(None, "fs", "tp"),
        P(None, "fs", "tp"),
        P(None, "fs", "tp"),
    )
    return jax.shard_map(
        body,
        mesh=mesh,
        in_specs=placed,
        out_specs=(
            P(("grp", "fs"), None, "tp"),
            P(("grp", "fs"), None, "tp"),
            P(("grp", "fs"), None, "tp"),
            P(("grp", "fs"), "tp"),
        ),
        check_vma=False,
    )
```

```python
import jax
import jax.numpy as jnp
from jax import lax
from jax.experimental import pallas as pl
from jax.experimental.pallas import tpu as pltpu
from jax.sharding import PartitionSpec as P

norm_epsilon = 1e-06


def slot_numbers(route_ids, experts, capacity):
    flat_ids = route_ids.reshape(-1)
    onehot = (flat_ids[:, None] == jnp.arange(experts, dtype=jnp.int32)[None, :]).astype(jnp.int32)
    before = jnp.cumsum(onehot, axis=0) - onehot
    position = jnp.sum(before * onehot, axis=1)
    return (flat_ids * capacity + position).reshape(route_ids.shape)


def local(tokens, route_ids, route_weights, norm_gain, gate_master, up_master, down_master):
    experts = gate_master.shape[0]
    shards = lax.axis_size("fs")
    columns = lax.axis_size("tp")
    per_device = experts // shards
    tok_rows = route_ids.shape[0]
    top_count = route_ids.shape[1]
    local_width = tokens.shape[1]
    model_width = local_width * columns
    capacity = max(2, 3 * tok_rows * top_count // (2 * experts))
    row_gain = norm_gain[None, :, None]
    gate_half = (gate_master * row_gain).astype(jnp.bfloat16)
    up_half = (up_master * row_gain).astype(jnp.bfloat16)
    down_half = down_master.astype(jnp.bfloat16)
    gate_serve, up_serve, down_serve = (
        lax.all_to_all(gate_half, "fs", split_axis=0, concat_axis=1, tiled=True),
        lax.all_to_all(up_half, "fs", split_axis=0, concat_axis=1, tiled=True),
        lax.all_to_all(down_half, "fs", split_axis=0, concat_axis=1, tiled=True),
    )
    slot_ids = slot_numbers(route_ids, experts, capacity)
    slot_range = jnp.arange(experts * capacity, dtype=jnp.int32)
    selects = [
        (slot_ids[:, rank_slot, None] == slot_range[None, :]).astype(jnp.bfloat16)
        for rank_slot in range(top_count)
    ]
    placing = selects[0]
    for extra in selects[1:]:
        placing = placing + extra
    local_values = tokens.astype(jnp.float32)
    squares = lax.psum(jnp.sum(local_values * local_values, axis=1), "tp")
    inverse = lax.rsqrt(squares / model_width + norm_epsilon)[:, None]
    normed = (local_values * inverse).astype(jnp.bfloat16)
    buffer = jnp.einsum("ts,td->sd", placing, normed, preferred_element_type=jnp.float32).astype(
        jnp.bfloat16
    )
    arrived = lax.all_to_all(
        buffer.reshape(shards, per_device * capacity, local_width),
        "fs",
        split_axis=0,
        concat_axis=0,
        tiled=True,
    )
    arrived = arrived.reshape(shards, per_device, capacity, local_width)
    partial_value = lax.all_gather(arrived, "tp", axis=3, tiled=True)
    gate_sum = jnp.einsum(
        "sxcd,xdf->xscf", partial_value, gate_serve, preferred_element_type=jnp.float32
    )
    up_sum = jnp.einsum(
        "sxcd,xdf->xscf", partial_value, up_serve, preferred_element_type=jnp.float32
    )
    hidden = (jax.nn.silu(gate_sum) * up_sum).astype(jnp.bfloat16)
    products = jnp.einsum("xdf,xscf->dsxc", down_serve, hidden, preferred_element_type=jnp.float32)
    summed = lax.psum_scatter(
        products.reshape(local_width * lax.axis_size("tp"), shards * per_device * capacity).astype(
            jnp.bfloat16
        ),
        "tp",
        scatter_dimension=0,
        tiled=True,
    )
    returned = lax.all_to_all(
        summed.reshape(local_width, shards, per_device * capacity),
        "fs",
        split_axis=1,
        concat_axis=1,
        tiled=True,
    )
    returned = returned.reshape(local_width, experts * capacity)
    combined = jnp.zeros((tok_rows, local_width), jnp.float32)
    for rank_slot in range(top_count):
        picked = jnp.einsum(
            "ts,ds->td", selects[rank_slot], returned, preferred_element_type=jnp.float32
        )
        combined = combined + route_weights[:, rank_slot : rank_slot + 1] * picked
    return (gate_serve, up_serve, down_serve, combined.astype(jnp.bfloat16))


MESH = pl.DeviceIdType.MESH
bf16, f32, i32 = jnp.bfloat16, jnp.float32, jnp.int32
GU_CUT, DN_CUT = 2, 4


def remote(src, dst, send, recv, to):
    return pltpu.make_async_remote_copy(
        src_ref=src, dst_ref=dst, send_sem=send, recv_sem=recv, device_id=to, device_id_type=MESH
    )


def kernel(
    tokens, ids_h, weights_h, gain_h, gm, um, dm,
    wgu, wd, moe,
    xt, ids, weights, gain, gcol, mv, sgu, sd, acc, inv, scale, wrow, wsend, hid,
    ss, sr, xs, xr, keep, zs, zr,
    in_sem, ld_sem, c_send, c_recv, w_send, w_recv, p_sib, p_x, p_recv,
    gu_send, gu_recv, guy_send, guy_recv, dn_send, dn_recv, dny_send, dny_recv,
    s_send, s_recv, x_send, x_recv, z_send, z_recv,
):
    g, f, t = lax.axis_index("grp"), lax.axis_index("fs"), lax.axis_index("tp")
    H, Fl = mv.shape[2:]
    Dl = 2 * H
    T, Dq = tokens.shape
    NT = xt.shape[0]
    D = NT * Dq
    Rg, Rd = H // GU_CUT, H // DN_CUT
    units = Dl // Fl
    per_half = units // 2
    pair, me = f // 2, lax.rem(f, 2)
    chip, core = t // 2, lax.rem(t, 2)
    mate = f + 1 - 2 * me
    twin = f + 2 - 4 * pair
    mate_twin = mate + 2 - 4 * pair
    far_a, far_b = 2 - pair, 3 - 3 * pair
    sib, over = {"tp": t + 1 - 2 * core}, {"tp": t + 2 - 4 * chip}
    peer, to_mate = {"grp": 1 - g}, {"fs": mate}
    mine_rows, mate_rows = (pl.ds(pl.multiple_of(i * T, T), T) for i in (me, 1 - me))
    inner = (f + 1) // 2 % 2 == 1
    home = chip == pair

    def cut(s, half, p, n):
        return pl.ds(pl.multiple_of(s * Dl + half * H + p * n, n), n)

    def both(s):
        return pl.ds(pl.multiple_of(s * Dl, Dl), Dl)

    small = [
        pltpu.make_async_copy(gain_h, gain, in_sem.at[0]),
        pltpu.make_async_copy(tokens, xt.at[t, mine_rows, :], in_sem.at[1]),
        pltpu.make_async_copy(ids_h, ids, in_sem.at[2]),
        pltpu.make_async_copy(weights_h, weights, in_sem.at[3]),
    ]
    for cp in small:
        cp.start()
    picks = [
        (1 - me, g), (1 - me + 2, g), (me, g), (me + 2, g), (me, 1 - g), (me + 2, 1 - g),
    ]
    loads = {}
    for k, m in [(k, m) for k in (0, 2, 1, 3) for m in (0, 1)] + [
        (k, 2) for k in (0, 1, 2, 3)
    ] + [(k, m) for k in (4, 5) for m in (0, 1, 2)]:
        e, half = picks[k]
        loads[k, m] = pltpu.make_async_copy(
            (gm, um, dm)[m].at[e, pl.ds(pl.multiple_of(half * H, H), H), :],
            mv.at[m, k], ld_sem.at[m, k],
        )
        loads[k, m].start()

    barrier = pltpu.get_barrier_semaphore()
    friends = [to_mate, {"fs": twin}, {"fs": mate_twin}, peer, sib, over]
    for who in friends:
        pl.semaphore_signal(barrier, inc=1, device_id=who, device_id_type=MESH)

    small[0].wait()
    gcol[...] = jnp.transpose(jnp.broadcast_to(gain[...], (Fl, Dl)))
    mine_half = pl.ds(pl.multiple_of(g * H, H), H)
    other_half = pl.ds(pl.multiple_of((1 - g) * H, H), H)
    small[2].wait()
    small[3].wait()
    wrow[me] = jnp.zeros(wsend.shape, f32)
    wsend[...] = jnp.zeros(wsend.shape, f32)
    for slot in range(2):
        for ref, parity in ((wrow.at[me], me), (wsend, 1 - me)):
            row = jnp.where(ids[...] == parity + 2 * slot, weights[...], 0.0)
            ref[slot : slot + 1, :T] = jnp.sum(row, axis=0, keepdims=True)
    small[1].wait()
    pl.semaphore_wait(barrier, len(friends))
    w_hop = remote(wsend, wrow.at[me], w_send, w_recv, to_mate)
    w_hop.start()


    def tok(q, rows):
        return xt.at[q, rows, :]

    token_hop = remote(tok(t, mine_rows), tok(t, mine_rows), c_send, c_recv, to_mate)
    token_hop.start()

    def spread(rows, i):
        block = tok(t, rows)
        remote(block, block, p_x.at[i], p_recv.at[t, i], over).start()
        remote(block, block, p_sib.at[t, i], p_recv.at[t, i], sib).start()

    def pass_on(rows, i):
        q = t + 2 - 4 * chip
        block = tok(q, rows)
        remote(block, block, p_recv.at[q, i], p_recv.at[q, i], sib).wait_recv()
        remote(block, block, p_sib.at[q, i], p_recv.at[q, i], sib).start()

    def sib_arrived(rows, i):
        for c in range(2):
            q = 2 * c + 1 - core
            block = tok(q, rows)
            remote(block, block, p_recv.at[q, i], p_recv.at[q, i], sib).wait_recv()

    spread(mine_rows, me)

    def gu_copy(kind, slot, p):
        src = (
            wgu.at[slot, cut(f, g, p, Rg), :] if kind == 0 else sgu.at[slot, p * Rg : (p + 1) * Rg, :]
        )
        return remote(
            src, wgu.at[slot, cut(f, g, p, Rg), :], gu_send.at[kind, slot, p],
            gu_recv.at[f, slot, p], {"fs": (twin, mate_twin, mate)[kind]},
        )

    def dn_copy(kind, p):
        src = wd.at[cut(f, g, p, Rd), :] if kind == 0 else sd.at[p * Rd : (p + 1) * Rd, :]
        return remote(
            src, wd.at[cut(f, g, p, Rd), :], dn_send.at[kind, p], dn_recv.at[f, p],
            {"fs": (twin, mate_twin, mate)[kind]},
        )

    def send_gu(slot, kinds):
        for p in range(GU_CUT):
            for kind in kinds:
                gu_copy(kind, slot, p).start()

    def send_dn(kinds):
        for p in range(DN_CUT):
            for kind in kinds:
                dn_copy(kind, p).start()

    def gu_ready(slot, k, dst, part):
        loads[k, 0].wait()
        loads[k, 1].wait()
        dst[:, :Fl] = (mv[0, k] * gcol[part, :]).astype(bf16)
        dst[:, Fl:] = (mv[1, k] * gcol[part, :]).astype(bf16)

    own_gu = [wgu.at[slot, cut(f, g, 0, H), :] for slot in range(2)]
    gu_ready(0, 0, sgu.at[0], mine_half)

    @pl.when(inner)
    def _():
        send_gu(0, (1, 2))

    @pl.when(jnp.logical_not(inner))
    def _():
        send_gu(0, (2,))

    gu_ready(0, 2, own_gu[0], mine_half)

    @pl.when(inner)
    def _():
        send_gu(0, (0,))

    gu_ready(1, 1, sgu.at[1], mine_half)

    @pl.when(inner)
    def _():
        send_gu(1, (1, 2))

    @pl.when(jnp.logical_not(inner))
    def _():
        send_gu(1, (2,))

    gu_ready(1, 3, own_gu[1], mine_half)

    @pl.when(inner)
    def _():
        send_gu(1, (0,))

    @pl.when(jnp.logical_not(inner))
    def _():
        send_gu(0, (0, 1))
        send_gu(1, (0, 1))

    for k in range(4):
        loads[k, 2].wait()
    for slot in range(2):
        lanes = slice(slot * Fl, (slot + 1) * Fl)
        sd[:, lanes] = mv[2, slot].astype(bf16)
        wd[cut(f, g, 0, H), lanes] = mv[2, 2 + slot].astype(bf16)
    send_dn((2,))

    @pl.when(jnp.logical_not(inner))
    def _():
        send_dn((0, 1))

    for slot in range(2):
        lanes = slice(slot * Fl, (slot + 1) * Fl)
        gu_ready(slot, 4 + slot, wgu.at[slot, cut(f, 1 - g, 0, H), :], other_half)
        loads[4 + slot, 2].wait()
        wd[cut(f, 1 - g, 0, H), lanes] = mv[2, 4 + slot].astype(bf16)

    def gu_forward(s, slot, p):
        here = wgu.at[slot, cut(s, g, p, Rg), :]
        remote(here, here, gu_recv.at[s, slot, p], gu_recv.at[s, slot, p], peer).wait_recv()
        remote(here, here, guy_send.at[s, slot, p], guy_recv.at[s, slot, p], peer).start()

    def gu_peer(s, slot):
        for p in range(GU_CUT):
            there = wgu.at[slot, cut(s, 1 - g, p, Rg), :]
            remote(there, there, guy_recv.at[s, slot, p], guy_recv.at[s, slot, p], peer).wait_recv()

    def dn_forward(s, p):
        here = wd.at[cut(s, g, p, Rd), :]
        remote(here, here, dn_recv.at[s, p], dn_recv.at[s, p], peer).wait_recv()
        remote(here, here, dny_send.at[s, p], dny_recv.at[s, p], peer).start()

    def dn_peer(s, p):
        there = wd.at[cut(s, 1 - g, p, Rd), :]
        remote(there, there, dny_recv.at[s, p], dny_recv.at[s, p], peer).wait_recv()

    def gu_all(s, slot):
        for p in range(GU_CUT):
            gu_forward(s, slot, p)

    def partial_sums(s, slot):
        return jnp.dot(xt[s], wgu[slot, both(s), :], preferred_element_type=f32)

    gu_all(far_a, 0)
    gu_all(far_a, 1)
    remote(tok(t, mate_rows), tok(t, mate_rows), c_send, c_recv, to_mate).wait_recv()
    spread(mate_rows, 1 - me)
    pass_on(mine_rows, me)
    gu_all(mate, 0)
    gu_all(far_b, 0)
    gu_all(mate, 1)
    pass_on(mate_rows, 1 - me)
    gu_forward(far_b, 1, 0)

    @pl.when(inner)
    def _():
        send_dn((0, 1))

    for p in range(1, GU_CUT):
        gu_forward(far_b, 1, p)

    remote(wsend, wrow.at[1 - me], w_recv, w_recv, to_mate).wait_recv()
    sib_arrived(mine_rows, me)
    sib_arrived(mate_rows, 1 - me)
    for i in range(2):
        rows = slice(i * T, (i + 1) * T)
        sq = jnp.zeros((T, Fl), f32)
        for q in range(NT):
            for c in range(Dq // Fl):
                part = xt[q, rows, c * Fl : (c + 1) * Fl].astype(f32)
                sq = sq + part * part
        root = lax.rsqrt(jnp.sum(sq, axis=1, keepdims=True) / D + norm_epsilon)
        inv[rows, :] = jnp.broadcast_to(root, (T, Fl))
        for slot in range(2):
            wide = jnp.transpose(
                jnp.broadcast_to(wrow[i, slot : slot + 1, :], (Fl, wrow.shape[2]))
            )
            scale[slot, rows, :] = wide[:T] * root

    for slot in range(2):
        acc[slot] = partial_sums(f, slot)
    for s in (far_a, mate):
        for slot in range(2):
            gu_peer(s, slot)
            acc[slot] += partial_sums(s, slot)

    ratio = DN_CUT // per_half

    def far_forward(j):
        for p in range(j * ratio, (j + 1) * ratio):
            dn_forward(far_a, p)
            dn_forward(far_b, p)

    def far_peer(j):
        for p in range(j * ratio, (j + 1) * ratio):
            dn_peer(far_a, p)
            dn_peer(far_b, p)

    def hidden(slot):
        gu_peer(far_b, slot)
        sums = acc[slot] + partial_sums(far_b, slot)
        gate, up = sums[:, :Fl] * inv[...], sums[:, Fl:] * scale[slot]
        hid[:, slot * Fl : (slot + 1) * Fl] = (gate / (1.0 + jnp.exp(-gate)) * up).astype(bf16)

    near_mine, near_theirs = 2 * pair + core, 2 * pair + 1 - core
    far_mine, far_theirs = 2 - 2 * pair + core, 2 - 2 * pair + 1 - core

    def out_part(s, u, n):
        rows = pl.ds(pl.multiple_of(s * Dl + u * Fl, Fl), n * Fl)
        return lax.dot_general(
            hid[...], wd[rows, :], (((1,), (1,)), ((), ())), preferred_element_type=f32
        )

    def swap(n, u, count):
        at = pl.ds(u, count)
        return remote(ss.at[n, at], sr.at[n, at], s_send.at[n, u], s_recv.at[n, u], sib)

    def cross(n, u, j):
        if x_first(j):
            return remote(xs.at[n, u], xr.at[n, u], x_send.at[n, u], x_recv.at[n, u], over)
        half = pl.ds(0, T)
        return remote(xs.at[n, u, half], xr.at[n, u, half], x_send.at[n, u], x_recv.at[n, u], over)

    def back(n, u):
        return remote(zs.at[n, u], zr.at[n, u], z_send.at[n, u], z_recv.at[n, u], to_mate)

    def x_first(j):
        return j % 2 == 0

    def is_kept(n):
        return home if n == 0 else jnp.logical_not(home)

    def theirs(n, s, u, count):
        y = out_part(s, u, count)
        for j in range(count):
            ss[n, u + j] = y[:, j * Fl : (j + 1) * Fl].astype(bf16)
        swap(n, u, count).start()

    def mine(n, s, u, j0, count):
        y = out_part(s, u, count)
        swap(n, u, count).wait_recv()
        for i in range(count):
            j, at = j0 + i, u + i
            keep[n, at] = y[:, i * Fl : (i + 1) * Fl] + sr[n, at].astype(f32)
            if x_first(j):
                @pl.when(jnp.logical_not(is_kept(n)))
                def _():
                    xs[n, at] = keep[n, at].astype(bf16)
                    cross(n, at, j).start()
            else:
                zs[n, at] = keep[n, at, mate_rows, :].astype(bf16)
                back(n, at).start()

    def own(n, u):
        return keep[n, u, mine_rows, :]

    def second(n, u, j):
        if x_first(j):
            @pl.when(is_kept(n))
            def _():
                cross(n, u, j).wait_recv()
                zs[n, u] = (keep[n, u, mate_rows, :] + xr[n, u, mate_rows, :].astype(f32)).astype(bf16)
                back(n, u).start()
        else:
            @pl.when(jnp.logical_not(is_kept(n)))
            def _():
                back(n, u).wait_recv()
                xs[n, u, :T] = (own(n, u) + zr[n, u].astype(f32)).astype(bf16)
                cross(n, u, j).start()

    def last(n, u, j):
        back(n, u).wait_recv()
        if x_first(j):
            other = xr[n, u, mine_rows, :]
        else:
            cross(n, u, j).wait_recv()
            other = xr[n, u, :T]
        lanes = pl.ds(pl.multiple_of(u * Fl, Fl), Fl)
        moe[:, lanes] = (own(n, u) + other.astype(f32) + zr[n, u].astype(f32)).astype(bf16)

    near_units = [(0, u, u % per_half) for u in range(units)]
    far_units = [(1, half * per_half + j, j) for half in (g, 1 - g) for j in range(per_half)]

    for p in range(DN_CUT):
        dn_forward(mate, p)
    hidden(0)
    far_forward(0)
    hidden(1)
    for p in range(DN_CUT):
        dn_peer(mate, p)
    for half in range(2):
        theirs(0, near_theirs, half * per_half, per_half)
    far_forward(1)
    for half in range(2):
        mine(0, near_mine, half * per_half, 0, per_half)
    for n, u, j in far_units[:per_half]:
        theirs(1, far_theirs, u, 1)
    for n, u, j in far_units[:per_half]:
        mine(1, far_mine, u, j, 1)
    for half, (n, u, j) in zip(range(per_half), far_units[per_half:]):
        far_peer(half)
        theirs(1, far_theirs, u, 1)
    for half, (n, u, j) in zip(range(per_half), far_units[per_half:]):
        mine(1, far_mine, u, j, 1)
    for half_units in near_units + far_units:
        second(*half_units)
    for half_units in far_units:
        @pl.when(jnp.logical_not(home))
        def _():
            last(*half_units)
    for half_units in near_units:
        @pl.when(home)
        def _():
            last(*half_units)

    token_hop.wait_send()
    w_hop.wait_send()
    for i, rows in ((me, mine_rows), (1 - me, mate_rows)):
        block = tok(t, rows)
        remote(block, block, p_x.at[i], p_x.at[i], over).wait_send()
        for q in (t, t + 2 - 4 * chip):
            remote(block, block, p_sib.at[q, i], p_sib.at[q, i], sib).wait_send()
    for kind in range(3):
        for slot in range(2):
            for p in range(GU_CUT):
                gu_copy(kind, slot, p).wait_send()
        for p in range(DN_CUT):
            dn_copy(kind, p).wait_send()
    for s in (mate, far_a, far_b):
        for slot in range(2):
            for p in range(GU_CUT):
                here = wgu.at[slot, cut(s, g, p, Rg), :]
                remote(here, here, guy_send.at[s, slot, p], guy_send.at[s, slot, p], peer).wait_send()
        for p in range(DN_CUT):
            here = wd.at[cut(s, g, p, Rd), :]
            remote(here, here, dny_send.at[s, p], dny_send.at[s, p], peer).wait_send()
    for half in range(2):
        swap(0, half * per_half, per_half).wait_send()
    for u in range(units):
        swap(1, u, 1).wait_send()
    for n in range(2):
        for u in range(units):
            j = u % per_half

            @pl.when(is_kept(n) | (not x_first(j)))
            def _():
                back(n, u).wait_send()

            @pl.when(jnp.logical_not(is_kept(n)))
            def _():
                cross(n, u, j).wait_send()


def finish_kernel(wgu, wd, moe, gate_o, up_o, down_o, moe_o, sems):
    Fl = gate_o.shape[2]
    slot = lax.axis_index("fs") // 2
    lanes = pl.ds(pl.multiple_of(slot * Fl, Fl), Fl)
    copies = [
        pltpu.make_async_copy(wgu.at[slot, :, :Fl], gate_o.at[0], sems.at[0]),
        pltpu.make_async_copy(wgu.at[slot, :, Fl:], up_o.at[0], sems.at[1]),
        pltpu.make_async_copy(wd.at[:, lanes], down_o.at[0], sems.at[2]),
        pltpu.make_async_copy(moe, moe_o, sems.at[3]),
    ]
    for cp in copies:
        cp.start()
    for cp in copies:
        cp.wait()


def fused(tokens, route_ids, route_weights, norm_gain, gate_master, up_master, down_master):
    NF, NT = lax.axis_size("fs"), lax.axis_size("tp")
    E, Dl, Fl = gate_master.shape
    T, Dq = tokens.shape
    K = route_ids.shape[1]
    H = Dl // 2
    D = Dl * NF
    Tw = -(-T // 128) * 128
    units = Dl // Fl
    dma = pltpu.SemaphoreType.DMA
    vmem, hbm = pl.BlockSpec(memory_space=pltpu.VMEM), pl.BlockSpec(memory_space=pl.ANY)
    gu, dn = (NF, 2, GU_CUT), (NF, DN_CUT)
    ins = (
        tokens, route_ids.T, route_weights.T, norm_gain[None, :],
        gate_master, up_master, down_master,
    )
    done = pl.pallas_call(
        kernel,
        out_shape=(
            pltpu.VMEM((2, D, 2 * Fl), bf16), pltpu.VMEM((D, 2 * Fl), bf16), pltpu.VMEM((T, Dq), bf16),
        ),
        in_specs=[hbm] * 7,
        out_specs=(vmem,) * 3,
        scratch_shapes=[
            pltpu.VMEM((NT, 2 * T, Dq), bf16),
            pltpu.VMEM((K, T), i32),
            pltpu.VMEM((K, T), f32),
            pltpu.VMEM((1, Dl), f32),
            pltpu.VMEM((Dl, Fl), f32),
            pltpu.VMEM((3, 6, H, Fl), f32),
            pltpu.VMEM((2, H, 2 * Fl), bf16),
            pltpu.VMEM((H, 2 * Fl), bf16),
            pltpu.VMEM((2, 2 * T, 2 * Fl), f32),
            pltpu.VMEM((2 * T, Fl), f32),
            pltpu.VMEM((2, 2 * T, Fl), f32),
            pltpu.VMEM((2, 8, Tw), f32),
            pltpu.VMEM((8, Tw), f32),
            pltpu.VMEM((2 * T, 2 * Fl), bf16),
            pltpu.VMEM((2, units, 2 * T, Fl), bf16),
            pltpu.VMEM((2, units, 2 * T, Fl), bf16),
            pltpu.VMEM((2, units, 2 * T, Fl), bf16),
            pltpu.VMEM((2, units, 2 * T, Fl), bf16),
            pltpu.VMEM((2, units, 2 * T, Fl), f32),
            pltpu.VMEM((2, units, T, Fl), bf16),
            pltpu.VMEM((2, units, T, Fl), bf16),
            dma((4,)), dma((3, 6)),
            dma(()), dma(()), dma(()), dma(()),
            dma((NT, 2)), dma((2,)), dma((NT, 2)),
            dma((3, 2, GU_CUT)), dma(gu), dma(gu), dma(gu),
            dma((3, DN_CUT)), dma(dn), dma(dn), dma(dn),
            dma((2, units)), dma((2, units)),
            dma((2, units)), dma((2, units)),
            dma((2, units)), dma((2, units)),
        ],
        compiler_params=pltpu.CompilerParams(
            collective_id=0, has_side_effects=True, vmem_limit_bytes=48 * 1024 * 1024
        ),
    )(*[pltpu.with_memory_space_constraint(a, pltpu.HBM) for a in ins])
    serve = jax.ShapeDtypeStruct((1, D, Fl), bf16)
    return pl.pallas_call(
        finish_kernel,
        out_shape=(serve, serve, serve, jax.ShapeDtypeStruct((T, Dq), bf16)),
        in_specs=[vmem] * 3,
        out_specs=(hbm,) * 4,
        scratch_shapes=[dma((4,))],
    )(*[pltpu.with_memory_space_constraint(a, pltpu.VMEM) for a in done])


def solution(mesh):
    shape = mesh.shape
    fits = shape['grp'] == 2 and shape['tp'] == shape['fs'] == 4
    body = fused if fits else local
    placed = (
        P(("grp", "fs"), "tp"),
        P(("grp", "fs"), None),
        P(("grp", "fs"), None),
        P("fs"),
        P(None, "fs", "tp"),
        P(None, "fs", "tp"),
        P(None, "fs", "tp"),
    )
    return jax.shard_map(
        body,
        mesh=mesh,
        in_specs=placed,
        out_specs=(
            P(("grp", "fs"), None, "tp"),
            P(("grp", "fs"), None, "tp"),
            P(("grp", "fs"), None, "tp"),
            P(("grp", "fs"), "tp"),
        ),
        check_vma=False,
    )
```

```python
import jax
import jax.numpy as jnp
from jax import lax
from jax.experimental import pallas as pl
from jax.experimental.pallas import tpu as pltpu
from jax.sharding import PartitionSpec as P

norm_epsilon = 1e-06


def slot_numbers(route_ids, experts, capacity):
    flat_ids = route_ids.reshape(-1)
    onehot = (flat_ids[:, None] == jnp.arange(experts, dtype=jnp.int32)[None, :]).astype(jnp.int32)
    before = jnp.cumsum(onehot, axis=0) - onehot
    position = jnp.sum(before * onehot, axis=1)
    return (flat_ids * capacity + position).reshape(route_ids.shape)


def local(tokens, route_ids, route_weights, norm_gain, gate_master, up_master, down_master):
    experts = gate_master.shape[0]
    shards = lax.axis_size("fs")
    columns = lax.axis_size("tp")
    per_device = experts // shards
    tok_rows = route_ids.shape[0]
    top_count = route_ids.shape[1]
    local_width = tokens.shape[1]
    model_width = local_width * columns
    capacity = max(2, 3 * tok_rows * top_count // (2 * experts))
    row_gain = norm_gain[None, :, None]
    gate_half = (gate_master * row_gain).astype(jnp.bfloat16)
    up_half = (up_master * row_gain).astype(jnp.bfloat16)
    down_half = down_master.astype(jnp.bfloat16)
    gate_serve, up_serve, down_serve = (
        lax.all_to_all(gate_half, "fs", split_axis=0, concat_axis=1, tiled=True),
        lax.all_to_all(up_half, "fs", split_axis=0, concat_axis=1, tiled=True),
        lax.all_to_all(down_half, "fs", split_axis=0, concat_axis=1, tiled=True),
    )
    slot_ids = slot_numbers(route_ids, experts, capacity)
    slot_range = jnp.arange(experts * capacity, dtype=jnp.int32)
    selects = [
        (slot_ids[:, rank_slot, None] == slot_range[None, :]).astype(jnp.bfloat16)
        for rank_slot in range(top_count)
    ]
    placing = selects[0]
    for extra in selects[1:]:
        placing = placing + extra
    local_values = tokens.astype(jnp.float32)
    squares = lax.psum(jnp.sum(local_values * local_values, axis=1), "tp")
    inverse = lax.rsqrt(squares / model_width + norm_epsilon)[:, None]
    normed = (local_values * inverse).astype(jnp.bfloat16)
    buffer = jnp.einsum("ts,td->sd", placing, normed, preferred_element_type=jnp.float32).astype(
        jnp.bfloat16
    )
    arrived = lax.all_to_all(
        buffer.reshape(shards, per_device * capacity, local_width),
        "fs",
        split_axis=0,
        concat_axis=0,
        tiled=True,
    )
    arrived = arrived.reshape(shards, per_device, capacity, local_width)
    partial_value = lax.all_gather(arrived, "tp", axis=3, tiled=True)
    gate_sum = jnp.einsum(
        "sxcd,xdf->xscf", partial_value, gate_serve, preferred_element_type=jnp.float32
    )
    up_sum = jnp.einsum(
        "sxcd,xdf->xscf", partial_value, up_serve, preferred_element_type=jnp.float32
    )
    hidden = (jax.nn.silu(gate_sum) * up_sum).astype(jnp.bfloat16)
    products = jnp.einsum("xdf,xscf->dsxc", down_serve, hidden, preferred_element_type=jnp.float32)
    summed = lax.psum_scatter(
        products.reshape(local_width * lax.axis_size("tp"), shards * per_device * capacity).astype(
            jnp.bfloat16
        ),
        "tp",
        scatter_dimension=0,
        tiled=True,
    )
    returned = lax.all_to_all(
        summed.reshape(local_width, shards, per_device * capacity),
        "fs",
        split_axis=1,
        concat_axis=1,
        tiled=True,
    )
    returned = returned.reshape(local_width, experts * capacity)
    combined = jnp.zeros((tok_rows, local_width), jnp.float32)
    for rank_slot in range(top_count):
        picked = jnp.einsum(
            "ts,ds->td", selects[rank_slot], returned, preferred_element_type=jnp.float32
        )
        combined = combined + route_weights[:, rank_slot : rank_slot + 1] * picked
    return (gate_serve, up_serve, down_serve, combined.astype(jnp.bfloat16))


MESH = pl.DeviceIdType.MESH
bf16, f32, i32 = jnp.bfloat16, jnp.float32, jnp.int32
GU_CUT, TOK_CUT = 2, 2
MATE_CUTS, FAR_CUTS = (2, 2), (4, 4, 4, 8, 8)


def remote(src, dst, send, recv, to):
    return pltpu.make_async_remote_copy(
        src_ref=src, dst_ref=dst, send_sem=send, recv_sem=recv, device_id=to, device_id_type=MESH
    )


def kernel(
    tokens, ids_h, weights_h, gain_h, gm, um, dm,
    wgu, wd, moe,
    xt, ids, weights, gain, gcol, mv, sgu, sd, acc, inv, scale, wrow, wsend, hid,
    ss, sr, xs, xr, keep, zs, zr,
    in_sem, ld_sem, sent, c_recv, w_recv, p_recv, gu_recv, guy_recv,
    mate_recv, mate_y, far_recv, far_y, s_recv, x_recv, z_recv,
):
    g, f, t = lax.axis_index("grp"), lax.axis_index("fs"), lax.axis_index("tp")
    H, Fl = mv.shape[2:]
    Dl = 2 * H
    T, Dq = tokens.shape
    NT = xt.shape[0]
    D = NT * Dq
    Rg = H // GU_CUT
    to_gu, to_dn, to_guy, to_dny, to_tok, to_w, to_tp, to_swap, to_x, to_z = (
        sent.at[i] for i in range(10)
    )
    units = Dl // Fl
    per_half = units // 2
    pair, me = f // 2, lax.rem(f, 2)
    chip, core = t // 2, lax.rem(t, 2)
    mate = f + 1 - 2 * me
    twin = f + 2 - 4 * pair
    mate_twin = mate + 2 - 4 * pair
    far_a, far_b = 2 - pair, 3 - 3 * pair
    sib, over = {"tp": t + 1 - 2 * core}, {"tp": t + 2 - 4 * chip}
    peer, to_mate = {"grp": 1 - g}, {"fs": mate}
    mine_rows, mate_rows = (pl.ds(pl.multiple_of(i * T, T), T) for i in (me, 1 - me))

    inner = (f + 1) // 2 % 2 == 1
    home = chip == pair
    own_mine = core == me

    def cut(s, half, p, n):
        return pl.ds(pl.multiple_of(s * Dl + half * H + p * n, n), n)

    def spans(cuts):
        at, out = 0, []
        for c in cuts:
            out.append((at, H // c))
            at += H // c
        return out

    mate_spans, far_spans = spans(MATE_CUTS), spans(FAR_CUTS)

    def span(s, half, at, n):
        return pl.ds(pl.multiple_of(s * Dl + half * H + at, n), n)

    is_inner = (f + 1) // 2 % 2
    kind_a, kind_b = is_inner, 1 - is_inner

    def both(s):
        return pl.ds(pl.multiple_of(s * Dl, Dl), Dl)

    small = [
        pltpu.make_async_copy(gain_h, gain, in_sem.at[0]),
        pltpu.make_async_copy(tokens, xt.at[t, mine_rows, :], in_sem.at[1]),
        pltpu.make_async_copy(ids_h, ids, in_sem.at[2]),
        pltpu.make_async_copy(weights_h, weights, in_sem.at[3]),
    ]
    for cp in small:
        cp.start()
    picks = [
        (1 - me, g), (1 - me + 2, g), (me, g), (me + 2, g), (me, 1 - g), (me + 2, 1 - g),
    ]
    loads = {}
    for k, m in [(k, m) for k in (0, 2, 1, 3) for m in (0, 1)] + [
        (k, 2) for k in (0, 1, 2, 3)
    ] + [(k, m) for k in (4, 5) for m in (0, 1, 2)]:
        e, half = picks[k]
        loads[k, m] = pltpu.make_async_copy(
            (gm, um, dm)[m].at[e, pl.ds(pl.multiple_of(half * H, H), H), :],
            mv.at[m, k], ld_sem.at[5 if k > 3 else 4 if m == 2 else k],
        )
        loads[k, m].start()

    barrier = pltpu.get_barrier_semaphore()
    friends = [to_mate, {"fs": twin}, {"fs": mate_twin}, peer, sib, over]
    for who in friends:
        pl.semaphore_signal(barrier, inc=1, device_id=who, device_id_type=MESH)

    small[0].wait()
    gcol[...] = jnp.transpose(jnp.broadcast_to(gain[...], (Fl, Dl)))
    mine_half = pl.ds(pl.multiple_of(g * H, H), H)
    other_half = pl.ds(pl.multiple_of((1 - g) * H, H), H)
    small[2].wait()
    small[3].wait()
    wrow[me] = jnp.zeros(wsend.shape, f32)
    wsend[...] = jnp.zeros(wsend.shape, f32)
    for slot in range(2):
        for ref, parity in ((wrow.at[me], me), (wsend, 1 - me)):
            row = jnp.where(ids[...] == parity + 2 * slot, weights[...], 0.0)
            ref[slot : slot + 1, :T] = jnp.sum(row, axis=0, keepdims=True)
    small[1].wait()
    pl.semaphore_wait(barrier, len(friends))
    w_hop = remote(wsend, wrow.at[me], to_w, w_recv, to_mate)
    w_hop.start()


    Tp = T // TOK_CUT

    def tok(q, i, p):
        return xt.at[q, pl.ds(pl.multiple_of(i * T + p * Tp, Tp), Tp), :]

    def token_hop(i, p):
        return remote(tok(t, i, p), tok(t, i, p), to_tok, c_recv.at[p], to_mate)

    def spread(i, p):
        block = tok(t, i, p)
        remote(block, block, to_tp, p_recv.at[0, i, p], over).start()
        remote(block, block, to_tp, p_recv.at[1, i, p], sib).start()

    def landed(way, q, i, p):
        block = tok(q, i, p)
        remote(block, block, to_tp, p_recv.at[way, i, p], sib).wait_recv()

    def pass_on(i):
        q = t + 2 - 4 * chip
        for p in range(TOK_CUT):
            landed(0, q, i, p)
            block = tok(q, i, p)
            remote(block, block, to_tp, p_recv.at[2, i, p], sib).start()

    def sib_arrived(i):
        for p in range(TOK_CUT):
            landed(1, t + 1 - 2 * core, i, p)
            landed(2, t + 2 - 4 * chip + 1 - 2 * core, i, p)

    def gu_copy(kind, slot, p):
        src = (
            wgu.at[slot, cut(f, g, p, Rg), :] if kind == 0 else sgu.at[slot, p * Rg : (p + 1) * Rg, :]
        )
        return remote(
            src, wgu.at[slot, cut(f, g, p, Rg), :], to_gu, gu_recv.at[kind, slot, p],
            {"fs": (twin, mate_twin, mate)[kind]},
        )

    def dn_copy(kind, p):
        at, n = (mate_spans if kind == 2 else far_spans)[p]
        there = wd.at[span(f, g, at, n), :]
        src = there if kind == 0 else sd.at[at : at + n, :]
        recv = mate_recv.at[p] if kind == 2 else far_recv.at[kind, p]
        return remote(src, there, to_dn, recv, {"fs": (twin, mate_twin, mate)[kind]})

    def send_gu(slot, kinds):
        for p in range(GU_CUT):
            for kind in kinds:
                gu_copy(kind, slot, p).start()

    def send_far():
        for p in range(len(far_spans)):
            for kind in (0, 1):
                dn_copy(kind, p).start()

    def send_mate():
        for p in range(len(mate_spans)):
            dn_copy(2, p).start()

    def loaded(block, i):
        pltpu.make_async_copy(block, block, ld_sem.at[i]).wait()

    def gu_ready(slot, k, dst, part):
        if k < 4:
            loaded(mv.at[:2, k], k)
        dst[:, :Fl] = (mv[0, k] * gcol[part, :]).astype(bf16)
        dst[:, Fl:] = (mv[1, k] * gcol[part, :]).astype(bf16)

    own_gu = [wgu.at[slot, cut(f, g, 0, H), :] for slot in range(2)]
    gu_ready(0, 0, sgu.at[0], mine_half)
    send_gu(0, (2,))
    for p in range(TOK_CUT):
        token_hop(me, p).start()
        spread(me, p)

    @pl.when(inner)
    def _():
        send_gu(0, (1,))

    gu_ready(0, 2, own_gu[0], mine_half)

    @pl.when(inner)
    def _():
        send_gu(0, (0,))

    gu_ready(1, 1, sgu.at[1], mine_half)
    send_gu(1, (2,))

    @pl.when(inner)
    def _():
        send_gu(1, (1,))

    gu_ready(1, 3, own_gu[1], mine_half)

    @pl.when(inner)
    def _():
        send_gu(1, (0,))

    @pl.when(jnp.logical_not(inner))
    def _():
        send_gu(0, (0, 1))
        send_gu(1, (0, 1))

    loaded(mv.at[2, :4], 4)
    for slot in range(2):
        lanes = slice(slot * Fl, (slot + 1) * Fl)
        sd[:, lanes] = mv[2, slot].astype(bf16)
        wd[cut(f, g, 0, H), lanes] = mv[2, 2 + slot].astype(bf16)
    send_mate()

    @pl.when(jnp.logical_not(inner))
    def _():
        send_far()

    loaded(mv.at[:, 4:], 5)
    for slot in range(2):
        lanes = slice(slot * Fl, (slot + 1) * Fl)
        gu_ready(slot, 4 + slot, wgu.at[slot, cut(f, 1 - g, 0, H), :], other_half)
        wd[cut(f, 1 - g, 0, H), lanes] = mv[2, 4 + slot].astype(bf16)

    def gu_forward(kind, slot, p):
        here = wgu.at[slot, cut(origin(kind), g, p, Rg), :]
        landing, onward = gu_recv.at[kind, slot, p], guy_recv.at[kind, slot, p]
        remote(here, here, to_guy, landing, peer).wait_recv()
        remote(here, here, to_guy, onward, peer).start()

    def gu_peer(kind, slot):
        for p in range(GU_CUT):
            there = wgu.at[slot, cut(origin(kind), 1 - g, p, Rg), :]
            remote(there, there, to_guy, guy_recv.at[kind, slot, p], peer).wait_recv()

    def origin(kind):
        return mate if isinstance(kind, int) else far_a if kind is kind_a else far_b

    def mate_forward():
        for p, (at, n) in enumerate(mate_spans):
            here = wd.at[span(mate, g, at, n), :]
            remote(here, here, to_dny, mate_recv.at[p], peer).wait_recv()
            remote(here, here, to_dny, mate_y.at[p], peer).start()

    def mate_peer():
        for p, (at, n) in enumerate(mate_spans):
            there = wd.at[span(mate, 1 - g, at, n), :]
            remote(there, there, to_dny, mate_y.at[p], peer).wait_recv()

    def far_forward(*pieces):
        for p in pieces:
            for kind, s in ((kind_a, far_a), (kind_b, far_b)):
                here = wd.at[span(s, g, *far_spans[p]), :]
                remote(here, here, to_dny, far_recv.at[kind, p], peer).wait_recv()
                remote(here, here, to_dny, far_y.at[kind, p], peer).start()

    def far_peer(*pieces):
        for p in pieces:
            for kind, s in ((kind_a, far_a), (kind_b, far_b)):
                there = wd.at[span(s, 1 - g, *far_spans[p]), :]
                remote(there, there, to_dny, far_y.at[kind, p], peer).wait_recv()

    def gu_all(kind, slot):
        for p in range(GU_CUT):
            gu_forward(kind, slot, p)

    def partial_sums(s, slot):
        return jnp.dot(xt[s], wgu[slot, both(s), :], preferred_element_type=f32)

    gu_all(2, 0)
    gu_all(kind_a, 0)
    gu_all(kind_a, 1)
    pass_on(me)
    for p in range(TOK_CUT):
        token_hop(1 - me, p).wait_recv()
        spread(1 - me, p)

    @pl.when(inner)
    def _():
        gu_all(2, 1)
        gu_all(kind_b, 0)
        pass_on(1 - me)
        gu_forward(kind_b, 1, 0)
        send_far()
        for p in range(1, GU_CUT):
            gu_forward(kind_b, 1, p)

    @pl.when(jnp.logical_not(inner))
    def _():
        gu_all(kind_b, 0)
        for p in range(GU_CUT):
            gu_forward(2, 1, p)
            if p == 0:
                pass_on(1 - me)
            gu_forward(kind_b, 1, p)

    remote(wsend, wrow.at[1 - me], w_recv, w_recv, to_mate).wait_recv()
    sib_arrived(me)
    sib_arrived(1 - me)
    for i in range(2):
        rows = slice(i * T, (i + 1) * T)
        sq = jnp.zeros((T, Fl), f32)
        for q in range(NT):
            for c in range(Dq // Fl):
                part = xt[q, rows, c * Fl : (c + 1) * Fl].astype(f32)
                sq = sq + part * part
        root = lax.rsqrt(jnp.sum(sq, axis=1, keepdims=True) / D + norm_epsilon)
        inv[rows, :] = jnp.broadcast_to(root, (T, Fl))
        for slot in range(2):
            wide = jnp.transpose(
                jnp.broadcast_to(wrow[i, slot : slot + 1, :], (Fl, wrow.shape[2]))
            )
            scale[slot, rows, :] = wide[:T] * root

    for slot in range(2):
        acc[slot] = partial_sums(f, slot)
    for kind, s in ((kind_a, far_a), (2, mate)):
        for slot in range(2):
            gu_peer(kind, slot)
            acc[slot] += partial_sums(s, slot)

    def hidden(slot):
        gu_peer(kind_b, slot)
        sums = acc[slot] + partial_sums(far_b, slot)
        gate, up = sums[:, :Fl] * inv[...], sums[:, Fl:] * scale[slot]
        hid[:, slot * Fl : (slot + 1) * Fl] = (gate / (1.0 + jnp.exp(-gate)) * up).astype(bf16)

    near_mine, near_theirs = 2 * pair + core, 2 * pair + 1 - core
    far_mine, far_theirs = 2 - 2 * pair + core, 2 - 2 * pair + 1 - core

    def out_part(s, u, n):
        rows = pl.ds(pl.multiple_of(s * Dl + u * Fl, Fl), n * Fl)
        return lax.dot_general(
            hid[...], wd[rows, :], (((1,), (1,)), ((), ())), preferred_element_type=f32
        )

    def swap(n, u, count, i):
        at = pl.ds(u, count)
        return remote(ss.at[n, at], sr.at[n, at], to_swap, s_recv.at[i], sib)

    def cross(n, u, count, rows, i):
        at = pl.ds(u, count)
        return remote(xs.at[n, at, :rows], xr.at[n, at, :rows], to_x, x_recv.at[i], over)

    def back(n, u, count, i):
        at = pl.ds(u, count)
        return remote(zs.at[n, at], zr.at[n, at], to_z, z_recv.at[i], to_mate)

    class Unit:
        def __init__(self, n, u, count, i, x_first):
            self.n, self.u, self.count, self.i, self.x_first = n, u, count, i, x_first
            self.theirs, self.mine = ((near_theirs, near_mine), (far_theirs, far_mine))[n]
            self.kept = home if n == 0 else jnp.logical_not(home)
            self.at = [u + c for c in range(count)]
            self.cross = cross(n, u, count, 2 * T if x_first else T, i)
            self.back = back(n, u, count, i)
            self.swap = swap(n, u, count, i)

        def give(self):
            y = out_part(self.theirs, self.u, self.count)
            for c, at in enumerate(self.at):
                ss[self.n, at] = y[:, c * Fl : (c + 1) * Fl].astype(bf16)
            self.swap.start()

        def sum(self):
            y = out_part(self.mine, self.u, self.count)
            self.swap.wait_recv()
            for c, at in enumerate(self.at):
                keep[self.n, at] = y[:, c * Fl : (c + 1) * Fl] + sr[self.n, at].astype(f32)

        def send(self):
            if self.x_first:
                @pl.when(jnp.logical_not(self.kept))
                def _():
                    for at in self.at:
                        xs[self.n, at] = keep[self.n, at].astype(bf16)
                    self.cross.start()
            else:
                for at in self.at:
                    zs[self.n, at] = keep[self.n, at, mate_rows, :].astype(bf16)
                self.back.start()

        def second(self):
            n = self.n
            if self.x_first:
                @pl.when(self.kept)
                def _():
                    self.cross.wait_recv()
                    for at in self.at:
                        zs[n, at] = (
                            keep[n, at, mate_rows, :] + xr[n, at, mate_rows, :].astype(f32)
                        ).astype(bf16)
                    self.back.start()
            else:
                @pl.when(jnp.logical_not(self.kept))
                def _():
                    self.back.wait_recv()
                    for at in self.at:
                        xs[n, at, :T] = (keep[n, at, mine_rows, :] + zr[n, at].astype(f32)).astype(bf16)
                    self.cross.start()

        def last(self):
            n = self.n

            @pl.when(self.kept)
            def _():
                self.back.wait_recv()
                if not self.x_first:
                    self.cross.wait_recv()
                for at in self.at:
                    other = xr[n, at, mine_rows, :] if self.x_first else xr[n, at, :T]
                    lanes = pl.ds(pl.multiple_of(at * Fl, Fl), Fl)
                    moe[:, lanes] = (
                        keep[n, at, mine_rows, :] + other.astype(f32) + zr[n, at].astype(f32)
                    ).astype(bf16)

    near = [Unit(0, half * per_half, per_half, half, half == 0) for half in range(2)]
    far = [
        Unit(1, half * per_half + j, 1, 2 + k * per_half + j, j % 2 == 0)
        for k, half in enumerate((g, 1 - g)) for j in range(per_half)
    ]
    pieces = range(len(far_spans))
    first_pieces = [p for p in pieces if far_spans[p][0] < H // 2]
    last_pieces = [p for p in pieces if p not in first_pieces]

    mate_forward()
    hidden(0)
    hidden(1)

    def near_give(mine_first):
        @pl.when(own_mine if mine_first else jnp.logical_not(own_mine))
        def _():
            for unit in near:
                unit.give()

    def near_sum(mine_first):
        @pl.when(own_mine if mine_first else jnp.logical_not(own_mine))
        def _():
            for unit in near:
                unit.sum()
            near[0].send()

    near_give(False)

    @pl.when(inner)
    def _():
        near_sum(True)
        mate_peer()
        near_give(True)
        far_forward(*first_pieces[:1])
        near_sum(False)
        far_forward(*first_pieces[1:])

    @pl.when(jnp.logical_not(inner))
    def _():
        far_forward(*first_pieces[:1])
        near_sum(True)
        far_forward(*first_pieces[1:])
        mate_peer()
        near_give(True)
        near_sum(False)

    far[0].give()
    far_forward(*last_pieces)
    near[1].send()
    far[1].give()
    far[0].sum()
    far[0].send()
    far_peer(*first_pieces)
    far[2].give()
    far[1].sum()
    far[1].send()
    far[2].sum()
    far[2].send()
    far_peer(*last_pieces)
    far[3].give()
    far[3].sum()
    far[3].send()
    for unit in near + far:
        unit.second()
    for unit in far + near:
        unit.last()

    def all_sent(block, sem):
        pltpu.make_async_copy(block, block, sem).wait()

    w_hop.wait_send()
    for block, sem in (
        (wgu.at[:, : 3 * H, :], to_gu), (wgu.at[:, : 3 * H, :], to_guy),
        (wd.at[: 3 * H, :], to_dn), (wd.at[: 3 * H, :], to_dny),
        (xt.at[0, :T, :], to_tok), (xt.at[:3], to_tp), (ss, to_swap),
        (xs.at[0, : 3 * units // 4], to_x), (zs.at[:, : 3 * units // 4], to_z),
    ):
        all_sent(block, sem)


def finish_kernel(wgu, wd, moe, gate_o, up_o, down_o, moe_o, sems):
    Fl = gate_o.shape[2]
    slot = lax.axis_index("fs") // 2
    lanes = pl.ds(pl.multiple_of(slot * Fl, Fl), Fl)
    copies = [
        pltpu.make_async_copy(wgu.at[slot, :, :Fl], gate_o.at[0], sems.at[0]),
        pltpu.make_async_copy(wgu.at[slot, :, Fl:], up_o.at[0], sems.at[1]),
        pltpu.make_async_copy(wd.at[:, lanes], down_o.at[0], sems.at[2]),
        pltpu.make_async_copy(moe, moe_o, sems.at[3]),
    ]
    for cp in copies:
        cp.start()
    for cp in copies:
        cp.wait()


def fused(tokens, route_ids, route_weights, norm_gain, gate_master, up_master, down_master):
    NF, NT = lax.axis_size("fs"), lax.axis_size("tp")
    E, Dl, Fl = gate_master.shape
    T, Dq = tokens.shape
    K = route_ids.shape[1]
    H = Dl // 2
    D = Dl * NF
    Tw = -(-T // 128) * 128
    units = Dl // Fl
    dma = pltpu.SemaphoreType.DMA
    vmem, hbm = pl.BlockSpec(memory_space=pltpu.VMEM), pl.BlockSpec(memory_space=pl.ANY)
    gu = (3, 2, GU_CUT)
    ins = (
        tokens, route_ids.T, route_weights.T, norm_gain[None, :],
        gate_master, up_master, down_master,
    )
    done = pl.pallas_call(
        kernel,
        out_shape=(
            pltpu.VMEM((2, D, 2 * Fl), bf16), pltpu.VMEM((D, 2 * Fl), bf16), pltpu.VMEM((T, Dq), bf16),
        ),
        in_specs=[hbm] * 7,
        out_specs=(vmem,) * 3,
        scratch_shapes=[
            pltpu.VMEM((NT, 2 * T, Dq), bf16),
            pltpu.VMEM((K, T), i32),
            pltpu.VMEM((K, T), f32),
            pltpu.VMEM((1, Dl), f32),
            pltpu.VMEM((Dl, Fl), f32),
            pltpu.VMEM((3, 6, H, Fl), f32),
            pltpu.VMEM((2, H, 2 * Fl), bf16),
            pltpu.VMEM((H, 2 * Fl), bf16),
            pltpu.VMEM((2, 2 * T, 2 * Fl), f32),
            pltpu.VMEM((2 * T, Fl), f32),
            pltpu.VMEM((2, 2 * T, Fl), f32),
            pltpu.VMEM((2, 8, Tw), f32),
            pltpu.VMEM((8, Tw), f32),
            pltpu.VMEM((2 * T, 2 * Fl), bf16),
            pltpu.VMEM((2, units, 2 * T, Fl), bf16),
            pltpu.VMEM((2, units, 2 * T, Fl), bf16),
            pltpu.VMEM((2, units, 2 * T, Fl), bf16),
            pltpu.VMEM((2, units, 2 * T, Fl), bf16),
            pltpu.VMEM((2, units, 2 * T, Fl), f32),
            pltpu.VMEM((2, units, T, Fl), bf16),
            pltpu.VMEM((2, units, T, Fl), bf16),
            dma((4,)), dma((6,)), dma((10,)),
            dma((TOK_CUT,)), dma(()), dma((3, 2, TOK_CUT)),
            dma(gu), dma(gu),
            dma((len(MATE_CUTS),)), dma((len(MATE_CUTS),)),
            dma((2, len(FAR_CUTS))), dma((2, len(FAR_CUTS))),
            dma((2 + units,)), dma((2 + units,)), dma((2 + units,)),
        ],
        compiler_params=pltpu.CompilerParams(
            collective_id=0, has_side_effects=True, vmem_limit_bytes=48 * 1024 * 1024
        ),
    )(*[pltpu.with_memory_space_constraint(a, pltpu.HBM) for a in ins])
    serve = jax.ShapeDtypeStruct((1, D, Fl), bf16)
    return pl.pallas_call(
        finish_kernel,
        out_shape=(serve, serve, serve, jax.ShapeDtypeStruct((T, Dq), bf16)),
        in_specs=[vmem] * 3,
        out_specs=(hbm,) * 4,
        scratch_shapes=[dma((4,))],
    )(*[pltpu.with_memory_space_constraint(a, pltpu.VMEM) for a in done])


def solution(mesh):
    shape = mesh.shape
    fits = shape['grp'] == 2 and shape['tp'] == shape['fs'] == 4
    body = fused if fits else local
    placed = (
        P(("grp", "fs"), "tp"),
        P(("grp", "fs"), None),
        P(("grp", "fs"), None),
        P("fs"),
        P(None, "fs", "tp"),
        P(None, "fs", "tp"),
        P(None, "fs", "tp"),
    )
    return jax.shard_map(
        body,
        mesh=mesh,
        in_specs=placed,
        out_specs=(
            P(("grp", "fs"), None, "tp"),
            P(("grp", "fs"), None, "tp"),
            P(("grp", "fs"), None, "tp"),
            P(("grp", "fs"), "tp"),
        ),
        check_vma=False,
    )
```

```python
import jax
import jax.numpy as jnp
from jax import lax
from jax.experimental import pallas as pl
from jax.experimental.pallas import tpu as pltpu
from jax.sharding import PartitionSpec as P

norm_epsilon = 1e-06


def slot_numbers(route_ids, experts, capacity):
    flat_ids = route_ids.reshape(-1)
    onehot = (flat_ids[:, None] == jnp.arange(experts, dtype=jnp.int32)[None, :]).astype(jnp.int32)
    before = jnp.cumsum(onehot, axis=0) - onehot
    position = jnp.sum(before * onehot, axis=1)
    return (flat_ids * capacity + position).reshape(route_ids.shape)


def local(tokens, route_ids, route_weights, norm_gain, gate_master, up_master, down_master):
    experts = gate_master.shape[0]
    shards = lax.axis_size("fs")
    columns = lax.axis_size("tp")
    per_device = experts // shards
    tok_rows = route_ids.shape[0]
    top_count = route_ids.shape[1]
    local_width = tokens.shape[1]
    model_width = local_width * columns
    capacity = max(2, 3 * tok_rows * top_count // (2 * experts))
    row_gain = norm_gain[None, :, None]
    gate_half = (gate_master * row_gain).astype(jnp.bfloat16)
    up_half = (up_master * row_gain).astype(jnp.bfloat16)
    down_half = down_master.astype(jnp.bfloat16)
    gate_serve, up_serve, down_serve = (
        lax.all_to_all(gate_half, "fs", split_axis=0, concat_axis=1, tiled=True),
        lax.all_to_all(up_half, "fs", split_axis=0, concat_axis=1, tiled=True),
        lax.all_to_all(down_half, "fs", split_axis=0, concat_axis=1, tiled=True),
    )
    slot_ids = slot_numbers(route_ids, experts, capacity)
    slot_range = jnp.arange(experts * capacity, dtype=jnp.int32)
    selects = [
        (slot_ids[:, rank_slot, None] == slot_range[None, :]).astype(jnp.bfloat16)
        for rank_slot in range(top_count)
    ]
    placing = selects[0]
    for extra in selects[1:]:
        placing = placing + extra
    local_values = tokens.astype(jnp.float32)
    squares = lax.psum(jnp.sum(local_values * local_values, axis=1), "tp")
    inverse = lax.rsqrt(squares / model_width + norm_epsilon)[:, None]
    normed = (local_values * inverse).astype(jnp.bfloat16)
    buffer = jnp.einsum("ts,td->sd", placing, normed, preferred_element_type=jnp.float32).astype(
        jnp.bfloat16
    )
    arrived = lax.all_to_all(
        buffer.reshape(shards, per_device * capacity, local_width),
        "fs",
        split_axis=0,
        concat_axis=0,
        tiled=True,
    )
    arrived = arrived.reshape(shards, per_device, capacity, local_width)
    partial_value = lax.all_gather(arrived, "tp", axis=3, tiled=True)
    gate_sum = jnp.einsum(
        "sxcd,xdf->xscf", partial_value, gate_serve, preferred_element_type=jnp.float32
    )
    up_sum = jnp.einsum(
        "sxcd,xdf->xscf", partial_value, up_serve, preferred_element_type=jnp.float32
    )
    hidden = (jax.nn.silu(gate_sum) * up_sum).astype(jnp.bfloat16)
    products = jnp.einsum("xdf,xscf->dsxc", down_serve, hidden, preferred_element_type=jnp.float32)
    summed = lax.psum_scatter(
        products.reshape(local_width * lax.axis_size("tp"), shards * per_device * capacity).astype(
            jnp.bfloat16
        ),
        "tp",
        scatter_dimension=0,
        tiled=True,
    )
    returned = lax.all_to_all(
        summed.reshape(local_width, shards, per_device * capacity),
        "fs",
        split_axis=1,
        concat_axis=1,
        tiled=True,
    )
    returned = returned.reshape(local_width, experts * capacity)
    combined = jnp.zeros((tok_rows, local_width), jnp.float32)
    for rank_slot in range(top_count):
        picked = jnp.einsum(
            "ts,ds->td", selects[rank_slot], returned, preferred_element_type=jnp.float32
        )
        combined = combined + route_weights[:, rank_slot : rank_slot + 1] * picked
    return (gate_serve, up_serve, down_serve, combined.astype(jnp.bfloat16))


MESH = pl.DeviceIdType.MESH
bf16, f32, i32 = jnp.bfloat16, jnp.float32, jnp.int32
GU_CUT, TOK_CUT = 2, 2
FAR_CUTS = (4, 4, 4, 8, 8)
NEAR_X, FAR_X = (True, False), (True, False, True, False)


def remote(src, dst, send, recv, to):
    return pltpu.make_async_remote_copy(
        src_ref=src, dst_ref=dst, send_sem=send, recv_sem=recv, device_id=to, device_id_type=MESH
    )


def kernel(
    tokens, ids_h, weights_h, gain_h, gm, um, dm,
    wgu, wd, moe,
    xt, ids, weights, gain, gcol, mv, mvd, sgu, sd, acc, inv, scale, wrow, wsend, hid,
    ss, sr, xs, xr, keep, zs, zr,
    in_sem, ld_sem, sent, c_recv, w_recv, p_recv, gu_recv, guy_recv,
    mate_recv, far_recv, far_y, s_recv, x_recv, z_recv,
):
    g, f, t = lax.axis_index("grp"), lax.axis_index("fs"), lax.axis_index("tp")
    H, Fl = mv.shape[2:]
    Dl = 2 * H
    T, Dq = tokens.shape
    NT = xt.shape[0]
    D = NT * Dq
    Rg = H // GU_CUT
    to_gu, to_dn, to_guy, to_dny, to_tok, to_w, to_tp, to_swap, to_x, to_z = (
        sent.at[i] for i in range(10)
    )
    units = Dl // Fl
    per_half = units // 2
    pair, me = f // 2, lax.rem(f, 2)
    chip, core = t // 2, lax.rem(t, 2)
    mate = f + 1 - 2 * me
    twin = f + 2 - 4 * pair
    mate_twin = mate + 2 - 4 * pair
    far_a, far_b = 2 - pair, 3 - 3 * pair
    sib, over = {"tp": t + 1 - 2 * core}, {"tp": t + 2 - 4 * chip}
    peer, to_mate = {"grp": 1 - g}, {"fs": mate}
    mine_rows, mate_rows = (pl.ds(pl.multiple_of(i * T, T), T) for i in (me, 1 - me))

    inner = (f + 1) // 2 % 2 == 1
    home = chip == pair
    own_mine = core == me

    def cut(s, half, p, n):
        return pl.ds(pl.multiple_of(s * Dl + half * H + p * n, n), n)

    def spans(cuts):
        at, out = 0, []
        for c in cuts:
            out.append((at, H // c))
            at += H // c
        return out

    far_spans = spans(FAR_CUTS)

    def span(s, half, at, n):
        return pl.ds(pl.multiple_of(s * Dl + half * H + at, n), n)

    is_inner = (f + 1) // 2 % 2
    kind_a, kind_b = is_inner, 1 - is_inner

    def both(s):
        return pl.ds(pl.multiple_of(s * Dl, Dl), Dl)

    small = [
        pltpu.make_async_copy(gain_h, gain, in_sem.at[0]),
        pltpu.make_async_copy(tokens, xt.at[t, mine_rows, :], in_sem.at[1]),
        pltpu.make_async_copy(ids_h, ids, in_sem.at[2]),
        pltpu.make_async_copy(weights_h, weights, in_sem.at[3]),
    ]
    for cp in small:
        cp.start()
    picks = [
        (1 - me, g), (1 - me + 2, g), (me, g), (me + 2, g), (me, 1 - g), (me + 2, 1 - g),
        (1 - me, 1 - g), (1 - me + 2, 1 - g),
    ]
    loads = {}
    for k, m in [(k, m) for k in (0, 2, 1, 3) for m in (0, 1)] + [
        (k, 2) for k in (0, 1, 2, 3, 6, 7)
    ] + [(k, m) for k in (4, 5) for m in (0, 1, 2)]:
        e, half = picks[k]
        loads[k, m] = pltpu.make_async_copy(
            (gm, um, dm)[m].at[e, pl.ds(pl.multiple_of(half * H, H), H), :],
            mvd.at[k - 6] if k > 5 else mv.at[m, k],
            ld_sem.at[6 if k > 5 else 5 if k > 3 else 4 if m == 2 else k],
        )
        loads[k, m].start()

    barrier = pltpu.get_barrier_semaphore()
    friends = [to_mate, {"fs": twin}, {"fs": mate_twin}, peer, sib, over]
    for who in friends:
        pl.semaphore_signal(barrier, inc=1, device_id=who, device_id_type=MESH)

    small[0].wait()
    gcol[...] = jnp.transpose(jnp.broadcast_to(gain[...], (Fl, Dl)))
    mine_half = pl.ds(pl.multiple_of(g * H, H), H)
    other_half = pl.ds(pl.multiple_of((1 - g) * H, H), H)
    small[2].wait()
    small[3].wait()
    wrow[me] = jnp.zeros(wsend.shape, f32)
    wsend[...] = jnp.zeros(wsend.shape, f32)
    for slot in range(2):
        for ref, parity in ((wrow.at[me], me), (wsend, 1 - me)):
            row = jnp.where(ids[...] == parity + 2 * slot, weights[...], 0.0)
            ref[slot : slot + 1, :T] = jnp.sum(row, axis=0, keepdims=True)
    small[1].wait()
    pl.semaphore_wait(barrier, len(friends))
    w_hop = remote(wsend, wrow.at[me], to_w, w_recv, to_mate)
    w_hop.start()


    Tp = T // TOK_CUT

    def tok(q, i, p):
        return xt.at[q, pl.ds(pl.multiple_of(i * T + p * Tp, Tp), Tp), :]

    def token_hop(i, p):
        return remote(tok(t, i, p), tok(t, i, p), to_tok, c_recv.at[p], to_mate)

    def spread(i, p):
        block = tok(t, i, p)
        remote(block, block, to_tp, p_recv.at[0, i, p], over).start()
        remote(block, block, to_tp, p_recv.at[1, i, p], sib).start()

    def landed(way, q, i, p):
        block = tok(q, i, p)
        remote(block, block, to_tp, p_recv.at[way, i, p], sib).wait_recv()

    def pass_on(i):
        q = t + 2 - 4 * chip
        for p in range(TOK_CUT):
            landed(0, q, i, p)
            block = tok(q, i, p)
            remote(block, block, to_tp, p_recv.at[2, i, p], sib).start()

    def sib_arrived(i):
        for p in range(TOK_CUT):
            landed(1, t + 1 - 2 * core, i, p)
            landed(2, t + 2 - 4 * chip + 1 - 2 * core, i, p)

    def gu_copy(kind, slot, p):
        src = (
            wgu.at[slot, cut(f, g, p, Rg), :] if kind == 0 else sgu.at[slot, p * Rg : (p + 1) * Rg, :]
        )
        return remote(
            src, wgu.at[slot, cut(f, g, p, Rg), :], to_gu, gu_recv.at[kind, slot, p],
            {"fs": (twin, mate_twin, mate)[kind]},
        )

    def dn_copy(kind, p):
        at, n = far_spans[p]
        there = wd.at[span(f, g, at, n), :]
        src = there if kind == 0 else sd.at[0, at : at + n, :]
        return remote(
            src, there, to_dn, far_recv.at[kind, p], {"fs": (twin, mate_twin)[kind]}
        )

    def mate_copy(i):
        half = (g, 1 - g)[i]
        return remote(sd.at[i], wd.at[span(f, half, 0, H), :], to_dny, mate_recv.at[i], to_mate)

    def send_gu(slot, kinds):
        for p in range(GU_CUT):
            for kind in kinds:
                gu_copy(kind, slot, p).start()

    def send_far():
        for p in range(len(far_spans)):
            for kind in (0, 1):
                dn_copy(kind, p).start()

    def send_mate():
        for i in range(2):
            mate_copy(i).start()

    def loaded(block, i):
        pltpu.make_async_copy(block, block, ld_sem.at[i]).wait()

    def gu_ready(slot, k, dst, part):
        if k < 4:
            loaded(mv.at[:2, k], k)
        dst[:, :Fl] = (mv[0, k] * gcol[part, :]).astype(bf16)
        dst[:, Fl:] = (mv[1, k] * gcol[part, :]).astype(bf16)

    own_gu = [wgu.at[slot, cut(f, g, 0, H), :] for slot in range(2)]
    gu_ready(0, 0, sgu.at[0], mine_half)
    send_gu(0, (2,))
    for p in range(TOK_CUT):
        token_hop(me, p).start()
        spread(me, p)

    @pl.when(inner)
    def _():
        send_gu(0, (1,))

    gu_ready(0, 2, own_gu[0], mine_half)

    @pl.when(inner)
    def _():
        send_gu(0, (0,))

    gu_ready(1, 1, sgu.at[1], mine_half)
    send_gu(1, (2,))

    @pl.when(inner)
    def _():
        send_gu(1, (1,))

    gu_ready(1, 3, own_gu[1], mine_half)

    @pl.when(inner)
    def _():
        send_gu(1, (0,))

    @pl.when(jnp.logical_not(inner))
    def _():
        send_gu(0, (0, 1))
        send_gu(1, (0, 1))

    loaded(mv.at[2, :4], 4)
    loaded(mvd, 6)
    for slot in range(2):
        lanes = slice(slot * Fl, (slot + 1) * Fl)
        sd[0, :, lanes] = mv[2, slot].astype(bf16)
        sd[1, :, lanes] = mvd[slot].astype(bf16)
        wd[cut(f, g, 0, H), lanes] = mv[2, 2 + slot].astype(bf16)
    send_mate()

    @pl.when(jnp.logical_not(inner))
    def _():
        send_far()

    loaded(mv.at[:, 4:], 5)
    for slot in range(2):
        lanes = slice(slot * Fl, (slot + 1) * Fl)
        gu_ready(slot, 4 + slot, wgu.at[slot, cut(f, 1 - g, 0, H), :], other_half)
        wd[cut(f, 1 - g, 0, H), lanes] = mv[2, 4 + slot].astype(bf16)

    def gu_forward(kind, slot, p):
        here = wgu.at[slot, cut(origin(kind), g, p, Rg), :]
        landing, onward = gu_recv.at[kind, slot, p], guy_recv.at[kind, slot, p]
        remote(here, here, to_guy, landing, peer).wait_recv()
        remote(here, here, to_guy, onward, peer).start()

    def gu_peer(kind, slot):
        for p in range(GU_CUT):
            there = wgu.at[slot, cut(origin(kind), 1 - g, p, Rg), :]
            remote(there, there, to_guy, guy_recv.at[kind, slot, p], peer).wait_recv()

    def origin(kind):
        return mate if isinstance(kind, int) else far_a if kind is kind_a else far_b

    def mate_arrived():
        for i, half in enumerate((g, 1 - g)):
            here = wd.at[span(mate, half, 0, H), :]
            remote(here, here, to_dny, mate_recv.at[i], to_mate).wait_recv()

    def far_forward(kind, *pieces):
        for p in pieces:
            here = wd.at[span(origin(kind), g, *far_spans[p]), :]
            remote(here, here, to_dny, far_recv.at[kind, p], peer).wait_recv()
            remote(here, here, to_dny, far_y.at[kind, p], peer).start()

    def far_peer(*pieces):
        for p in pieces:
            for kind, s in ((kind_a, far_a), (kind_b, far_b)):
                there = wd.at[span(s, 1 - g, *far_spans[p]), :]
                remote(there, there, to_dny, far_y.at[kind, p], peer).wait_recv()

    def gu_all(kind, slot):
        for p in range(GU_CUT):
            gu_forward(kind, slot, p)

    def partial_sums(s, slot):
        return jnp.dot(xt[s], wgu[slot, both(s), :], preferred_element_type=f32)

    gu_all(2, 0)
    gu_all(kind_a, 0)
    gu_all(kind_a, 1)
    pass_on(me)
    for p in range(TOK_CUT):
        token_hop(1 - me, p).wait_recv()
        spread(1 - me, p)

    @pl.when(inner)
    def _():
        gu_all(2, 1)
        gu_all(kind_b, 0)
        pass_on(1 - me)
        gu_forward(kind_b, 1, 0)
        send_far()
        for p in range(1, GU_CUT):
            gu_forward(kind_b, 1, p)

    @pl.when(jnp.logical_not(inner))
    def _():
        gu_all(kind_b, 0)
        for p in range(GU_CUT):
            gu_forward(2, 1, p)
            if p == 0:
                pass_on(1 - me)
            gu_forward(kind_b, 1, p)

    remote(wsend, wrow.at[1 - me], w_recv, w_recv, to_mate).wait_recv()
    sib_arrived(me)
    sib_arrived(1 - me)
    for i in range(2):
        rows = slice(i * T, (i + 1) * T)
        sq = jnp.zeros((T, Fl), f32)
        for q in range(NT):
            for c in range(Dq // Fl):
                part = xt[q, rows, c * Fl : (c + 1) * Fl].astype(f32)
                sq = sq + part * part
        root = lax.rsqrt(jnp.sum(sq, axis=1, keepdims=True) / D + norm_epsilon)
        inv[rows, :] = jnp.broadcast_to(root, (T, Fl))
        for slot in range(2):
            wide = jnp.transpose(
                jnp.broadcast_to(wrow[i, slot : slot + 1, :], (Fl, wrow.shape[2]))
            )
            scale[slot, rows, :] = wide[:T] * root

    for slot in range(2):
        acc[slot] = partial_sums(f, slot)
    for kind, s in ((kind_a, far_a), (2, mate)):
        for slot in range(2):
            gu_peer(kind, slot)
            acc[slot] += partial_sums(s, slot)

    def hidden(slot):
        gu_peer(kind_b, slot)
        sums = acc[slot] + partial_sums(far_b, slot)
        gate, up = sums[:, :Fl] * inv[...], sums[:, Fl:] * scale[slot]
        hid[:, slot * Fl : (slot + 1) * Fl] = (gate / (1.0 + jnp.exp(-gate)) * up).astype(bf16)

    near_mine, near_theirs = 2 * pair + core, 2 * pair + 1 - core
    far_mine, far_theirs = 2 - 2 * pair + core, 2 - 2 * pair + 1 - core

    def out_part(s, u, n):
        rows = pl.ds(pl.multiple_of(s * Dl + u * Fl, Fl), n * Fl)
        return lax.dot_general(
            hid[...], wd[rows, :], (((1,), (1,)), ((), ())), preferred_element_type=f32
        )

    def swap(n, u, count, i):
        at = pl.ds(u, count)
        return remote(ss.at[n, at], sr.at[n, at], to_swap, s_recv.at[i], sib)

    def cross(n, u, count, rows, i):
        at = pl.ds(u, count)
        return remote(xs.at[n, at, :rows], xr.at[n, at, :rows], to_x, x_recv.at[i], over)

    def back(n, u, count, i):
        at = pl.ds(u, count)
        return remote(zs.at[n, at], zr.at[n, at], to_z, z_recv.at[i], to_mate)

    class Unit:
        def __init__(self, n, u, count, i, x_first):
            self.n, self.u, self.count, self.x_first = n, u, count, x_first
            self.theirs, self.mine = ((near_theirs, near_mine), (far_theirs, far_mine))[n]
            self.kept = home if n == 0 else jnp.logical_not(home)
            self.at = [u + c for c in range(count)]
            rows = 2 * T if x_first else T
            self.cross = [cross(n, at, 1, rows, i + c) for c, at in enumerate(self.at)]
            self.back = [back(n, at, 1, i + c) for c, at in enumerate(self.at)]
            self.swap = swap(n, u, count, i)

        def give(self):
            y = out_part(self.theirs, self.u, self.count)
            for c, at in enumerate(self.at):
                ss[self.n, at] = y[:, c * Fl : (c + 1) * Fl].astype(bf16)
            self.swap.start()

        def sum(self):
            y = out_part(self.mine, self.u, self.count)
            self.swap.wait_recv()
            for c, at in enumerate(self.at):
                keep[self.n, at] = y[:, c * Fl : (c + 1) * Fl] + sr[self.n, at].astype(f32)

        def send(self):
            for at, over_x, over_z in zip(self.at, self.cross, self.back):
                if self.x_first:
                    @pl.when(jnp.logical_not(self.kept))
                    def _():
                        xs[self.n, at] = keep[self.n, at].astype(bf16)
                        over_x.start()
                else:
                    zs[self.n, at] = keep[self.n, at, mate_rows, :].astype(bf16)
                    over_z.start()

        def second(self, c=0):
            n, at, over_x, over_z = self.n, self.at[c], self.cross[c], self.back[c]
            if self.x_first:
                @pl.when(self.kept)
                def _():
                    over_x.wait_recv()
                    zs[n, at] = (
                        keep[n, at, mate_rows, :] + xr[n, at, mate_rows, :].astype(f32)
                    ).astype(bf16)
                    over_z.start()
            else:
                @pl.when(jnp.logical_not(self.kept))
                def _():
                    over_z.wait_recv()
                    xs[n, at, :T] = (keep[n, at, mine_rows, :] + zr[n, at].astype(f32)).astype(bf16)
                    over_x.start()

        def last(self):
            n = self.n

            @pl.when(self.kept)
            def _():
                for at, over_x, over_z in zip(self.at, self.cross, self.back):
                    over_z.wait_recv()
                    if not self.x_first:
                        over_x.wait_recv()
                    other = xr[n, at, mine_rows, :] if self.x_first else xr[n, at, :T]
                    lanes = pl.ds(pl.multiple_of(at * Fl, Fl), Fl)
                    moe[:, lanes] = (
                        keep[n, at, mine_rows, :] + other.astype(f32) + zr[n, at].astype(f32)
                    ).astype(bf16)

    near = [Unit(0, half * per_half, per_half, half * per_half, NEAR_X[half]) for half in range(2)]
    far = [
        Unit(1, half * per_half + j, 1, units + k * per_half + j, FAR_X[k * per_half + j])
        for k, half in enumerate((g, 1 - g)) for j in range(per_half)
    ]
    pieces = range(len(far_spans))
    first_pieces = [p for p in pieces if far_spans[p][0] < H // 2]
    last_pieces = [p for p in pieces if p not in first_pieces]

    def near_give(mine_first):
        @pl.when(own_mine if mine_first else jnp.logical_not(own_mine))
        def _():
            for unit in near:
                unit.give()

    def near_sum(mine_first):
        @pl.when(own_mine if mine_first else jnp.logical_not(own_mine))
        def _():
            for unit in near:
                unit.sum()
            for unit in near:
                if unit.x_first:
                    unit.send()

    hidden(0)
    hidden(1)
    near_give(False)
    far_forward(kind_a, 0, 1)

    @pl.when(inner)
    def _():
        near_sum(True)
        mate_arrived()
        near_give(True)
        far_forward(kind_a, 2, 3, 4)
        near_sum(False)
        far_forward(kind_b, 0, 1)

    @pl.when(jnp.logical_not(inner))
    def _():
        far_forward(kind_b, 0)
        near_sum(True)
        far_forward(kind_b, 1)
        far_forward(kind_a, 2, 3, 4)
        mate_arrived()
        near_give(True)
        far_forward(kind_b, 2)
        near_sum(False)
        far_forward(kind_b, 3)

    far[0].give()

    @pl.when(inner)
    def _():
        far_forward(kind_b, 2, 3)

    far_forward(kind_b, 4)
    for unit in near:
        if not unit.x_first:
            unit.send()
    far[1].give()
    far[0].sum()
    far[0].send()
    far_peer(*first_pieces)
    far[2].give()
    far[1].sum()
    far[1].send()
    far[2].sum()
    far[2].send()
    far_peer(*last_pieces)
    far[3].give()
    far[3].sum()
    far[3].send()
    near[0].second(0)
    near[1].second(0)
    near[1].second(1)
    near[0].second(1)
    for unit in far:
        unit.second()
    for unit in far + near:
        unit.last()

    def all_sent(block, sem):
        pltpu.make_async_copy(block, block, sem).wait()

    w_hop.wait_send()
    for block, sem in (
        (wgu.at[:, : 3 * H, :], to_gu), (wgu.at[:, : 3 * H, :], to_guy),
        (wd.at[: 2 * H, :], to_dn), (wd.at[: 4 * H, :], to_dny),
        (xt.at[0, :T, :], to_tok), (xt.at[:3], to_tp), (ss, to_swap),
    ):
        all_sent(block, sem)

    near_x, far_x = per_half * sum(NEAR_X), sum(FAR_X)

    def blocks(k):
        return xt.at[0, : k * T * Fl // Dq, :]

    @pl.when(home)
    def _():
        all_sent(blocks(units + far_x), to_x)
        all_sent(blocks(2 * units - far_x), to_z)

    @pl.when(jnp.logical_not(home))
    def _():
        all_sent(blocks(units + near_x), to_x)
        all_sent(blocks(2 * units - near_x), to_z)


def finish_kernel(wgu, wd, moe, gate_o, up_o, down_o, moe_o, sems):
    Fl = gate_o.shape[2]
    slot = lax.axis_index("fs") // 2
    lanes = pl.ds(pl.multiple_of(slot * Fl, Fl), Fl)
    copies = [
        pltpu.make_async_copy(wgu.at[slot, :, :Fl], gate_o.at[0], sems.at[0]),
        pltpu.make_async_copy(wgu.at[slot, :, Fl:], up_o.at[0], sems.at[1]),
        pltpu.make_async_copy(wd.at[:, lanes], down_o.at[0], sems.at[2]),
        pltpu.make_async_copy(moe, moe_o, sems.at[3]),
    ]
    for cp in copies:
        cp.start()
    for cp in copies:
        cp.wait()


def fused(tokens, route_ids, route_weights, norm_gain, gate_master, up_master, down_master):
    NF, NT = lax.axis_size("fs"), lax.axis_size("tp")
    E, Dl, Fl = gate_master.shape
    T, Dq = tokens.shape
    K = route_ids.shape[1]
    H = Dl // 2
    D = Dl * NF
    Tw = -(-T // 128) * 128
    units = Dl // Fl
    dma = pltpu.SemaphoreType.DMA
    vmem, hbm = pl.BlockSpec(memory_space=pltpu.VMEM), pl.BlockSpec(memory_space=pl.ANY)
    gu = (3, 2, GU_CUT)
    ins = (
        tokens, route_ids.T, route_weights.T, norm_gain[None, :],
        gate_master, up_master, down_master,
    )
    done = pl.pallas_call(
        kernel,
        out_shape=(
            pltpu.VMEM((2, D, 2 * Fl), bf16), pltpu.VMEM((D, 2 * Fl), bf16), pltpu.VMEM((T, Dq), bf16),
        ),
        in_specs=[hbm] * 7,
        out_specs=(vmem,) * 3,
        scratch_shapes=[
            pltpu.VMEM((NT, 2 * T, Dq), bf16),
            pltpu.VMEM((K, T), i32),
            pltpu.VMEM((K, T), f32),
            pltpu.VMEM((1, Dl), f32),
            pltpu.VMEM((Dl, Fl), f32),
            pltpu.VMEM((3, 6, H, Fl), f32),
            pltpu.VMEM((2, H, Fl), f32),
            pltpu.VMEM((2, H, 2 * Fl), bf16),
            pltpu.VMEM((2, H, 2 * Fl), bf16),
            pltpu.VMEM((2, 2 * T, 2 * Fl), f32),
            pltpu.VMEM((2 * T, Fl), f32),
            pltpu.VMEM((2, 2 * T, Fl), f32),
            pltpu.VMEM((2, 8, Tw), f32),
            pltpu.VMEM((8, Tw), f32),
            pltpu.VMEM((2 * T, 2 * Fl), bf16),
            pltpu.VMEM((2, units, 2 * T, Fl), bf16),
            pltpu.VMEM((2, units, 2 * T, Fl), bf16),
            pltpu.VMEM((2, units, 2 * T, Fl), bf16),
            pltpu.VMEM((2, units, 2 * T, Fl), bf16),
            pltpu.VMEM((2, units, 2 * T, Fl), f32),
            pltpu.VMEM((2, units, T, Fl), bf16),
            pltpu.VMEM((2, units, T, Fl), bf16),
            dma((4,)), dma((7,)), dma((10,)),
            dma((TOK_CUT,)), dma(()), dma((3, 2, TOK_CUT)),
            dma(gu), dma(gu),
            dma((2,)),
            dma((2, len(FAR_CUTS))), dma((2, len(FAR_CUTS))),
            dma((2 * units,)), dma((2 * units,)), dma((2 * units,)),
        ],
        compiler_params=pltpu.CompilerParams(
            collective_id=0, has_side_effects=True, vmem_limit_bytes=48 * 1024 * 1024
        ),
    )(*[pltpu.with_memory_space_constraint(a, pltpu.HBM) for a in ins])
    serve = jax.ShapeDtypeStruct((1, D, Fl), bf16)
    return pl.pallas_call(
        finish_kernel,
        out_shape=(serve, serve, serve, jax.ShapeDtypeStruct((T, Dq), bf16)),
        in_specs=[vmem] * 3,
        out_specs=(hbm,) * 4,
        scratch_shapes=[dma((4,))],
    )(*[pltpu.with_memory_space_constraint(a, pltpu.VMEM) for a in done])


def solution(mesh):
    shape = mesh.shape
    fits = shape['grp'] == 2 and shape['tp'] == shape['fs'] == 4
    body = fused if fits else local
    placed = (
        P(("grp", "fs"), "tp"),
        P(("grp", "fs"), None),
        P(("grp", "fs"), None),
        P("fs"),
        P(None, "fs", "tp"),
        P(None, "fs", "tp"),
        P(None, "fs", "tp"),
    )
    return jax.shard_map(
        body,
        mesh=mesh,
        in_specs=placed,
        out_specs=(
            P(("grp", "fs"), None, "tp"),
            P(("grp", "fs"), None, "tp"),
            P(("grp", "fs"), None, "tp"),
            P(("grp", "fs"), "tp"),
        ),
        check_vma=False,
    )
```
